32 devices in a mesh: grp: 2 (over x), sp: 4 (over y, core), tp: 4 (over z).
Axes of the slice: x: 2, y: 2, z: 4, core: 2. Of those that a mesh axis runs over, the one named last changes fastest.
Arguments:
- residual: bfloat16 [4096, 2048], P(('grp', 'sp', 'tp')), parts along dimension 0, may hold values from -6 to 6
- grouped_value_heads: bfloat16 [4096, 2, 1024], P(('grp', 'sp'), None, 'tp'), parts along dimension 0, may hold values from -6 to 6
- output_gate_heads: bfloat16 [4096, 2, 1024], P(('grp', 'sp'), None, 'tp'), parts along dimension 0, may hold values from -6 to 6
- projected_key_query: bfloat16 [4096, 384], P(('grp', 'sp')), parts along dimension 0, may hold values from -6 to 6
- raw_step_size: bfloat16 [4096, 2, 16], P(('grp', 'sp'), None, 'tp'), parts along dimension 0, may hold values from -3 to 3
- step_size_bias: float32 [2, 16], P(None, 'tp'), may hold values from -1 to 0.5
- head_decay_logarithm: float32 [2, 16], P(None, 'tp'), may hold values from -16 to -2
- position_extra_decay: float32 [4096], P(('grp', 'sp')), parts along dimension 0, may hold values from -0.7 to 0
- head_skip_weight: float32 [2, 16], P(None, 'tp'), may hold values from 0.5 to 2
- value_kernel_taps: bfloat16 [4, 2, 1024], P(None, None, 'tp'), may hold values from -3 to 3
- key_query_kernel: bfloat16 [4, 384], replicated, may hold values from -3 to 3
- head_norm_gain: float32 [2, 1024], P(None, 'tp'), may hold values from 0.1 to 1.9
- output_matrix: bfloat16 [2, 1024, 2048], P(None, 'tp'), may hold values from -0.125 to 0.125
- expert_norm_gain: float32 [2048], replicated, may hold values from 0.1 to 1.9
- expert_gate_weight: bfloat16 [4, 2048, 4096], P('sp', None, 'tp'), may hold values from -0.125 to 0.125
- expert_up_weight: bfloat16 [4, 2048, 4096], P('sp', None, 'tp'), may hold values from -0.125 to 0.125
- expert_down_weight: bfloat16 [4, 4096, 2048], P('sp', 'tp'), may hold values from -0.09375 to 0.09375
- token_expert_choice: int32 [4096, 2], P(('grp', 'sp', 'tp')), parts along dimension 0, may hold values from 0 to 3, all different within a row; in each aligned block of 128 rows (0 to 127, 128 to 255, ...) at most 65 rows name the same one
- expert_output_weight: float32 [4096, 2], P(('grp', 'sp', 'tp')), parts along dimension 0, may hold values from 0.2 to 1
Outputs:
- layer_out: bfloat16 [4096, 2048], P(('grp', 'sp', 'tp')), parts along dimension 0
The draws below stay inside these ranges and needn't reach their ends.
There are 2 independent parts, one for each index of `grp`. The reference program is written for one: setup_inputs(seed, part) draws one part's arguments, and reference() takes and returns one part's arrays. A program takes and returns all parts, laid end to end along the dimension named above; an argument that names none is the same for every part. Nothing has to cross between parts.
Inputs may be any that keep to these rules, and one draw needn't show every extreme that they name: `token_expert_choice`: each row names two different experts. The token rows of one device name one expert at most 65 times.
All inputs are finite; a program needn't handle non-finite values.
Results may differ from the reference program's by a relative error of at most 0.015.
Values may be sent and summed in bfloat16 or wider, within the bound.
No kernel may reach another device: no remote copies, remote signals or barrier semaphores. Data moves between devices by JAX's collectives and lax.ppermute only.
A program may use at most 128 MiB of HBM per device.

```python
import math
import jax
import jax.numpy as jnp
import numpy as np
from jax import lax

D = 2048
FF = 4096
GROUP_HEADS = 16
HEAD_DIM = 64
STATE_ONE = 64
STATE_TWO = 128
TAPS = 4
BLOCK = 128
ROWS_DEV = 128
SEQ_DEV = 512
TOKENS = 2048
EXPERTS = 4
CAP = 65
N_TP = 4


def draw_raw_step_size(key, part):
    first, second, third = jax.random.split(jax.random.fold_in(key, 11), 3)
    segments = TOKENS // SEQ_DEV
    blocks = TOKENS // BLOCK
    segment_shift = jax.random.uniform(first, (segments, 1), jnp.float32, -1.0, 1.0)
    segment_shift = jnp.repeat(segment_shift, SEQ_DEV // BLOCK, axis=0)
    block_shift = jax.random.uniform(second, (blocks, 1), jnp.float32, -0.5, 0.5)
    grid_shape = (blocks, BLOCK * 2 * GROUP_HEADS)
    jitter = jnp.clip(0.6 * jax.random.normal(third, grid_shape, jnp.float32), -1.5, 1.5)
    return (segment_shift + block_shift + jitter).reshape(TOKENS, 2, GROUP_HEADS).astype(jnp.bfloat16)


def draw_head_decay_logarithm(key, part):
    first, second = jax.random.split(jax.random.fold_in(key, 23))
    slow_share = 0.5
    choose_slow = jax.random.uniform(first, (2, GROUP_HEADS), jnp.float32) < slow_share
    level = jax.random.uniform(second, (2, GROUP_HEADS), jnp.float32, 0.0, 1.0)
    slow_rate = jnp.log(0.3 / TOKENS) + level * jnp.log(5.0)
    fast_rate = jnp.log(0.03) + level * jnp.log(3.0)
    return jnp.where(choose_slow, slow_rate, fast_rate).astype(jnp.float32)


def draw_position_extra_decay(key, part):
    first, second = jax.random.split(jax.random.fold_in(key, 37))
    spots = jax.random.randint(first, (3,), 0, TOKENS)
    depth = jax.random.uniform(second, (3,), jnp.float32, jnp.log(0.5), jnp.log(0.8))
    places = jnp.arange(TOKENS)
    struck = places[:, None] == spots[None, :]
    return jnp.sum(jnp.where(struck, depth[None, :], 0.0), axis=1).astype(jnp.float32)


def block_levels(stream_key, extent, cuts, least, largest):
    def one(axis_at, blocks):
        steps = jax.random.uniform(jax.random.fold_in(jax.random.fold_in(stream_key, 6), axis_at), (blocks,), jnp.float32, least / len(cuts), largest / len(cuts))
        return jnp.repeat(jnp.exp(steps), extent[axis_at] // blocks).reshape((-1,) + (1,) * (len(extent) - axis_at - 1))

    loudness = one(*cuts[0])
    for cut in cuts[1:]:
        loudness = loudness * one(*cut)
    return loudness


def deal_out(own_key, own, number, rows, number_of, top, reach, lean):
    ranking = jax.random.permutation(own_key, number_of)
    heavy_load, ordinary = load_shares(number_of, rows * top, reach, lean, True), load_shares(number_of, rows * top, reach, lean, False)
    places = jnp.arange(number_of)

    def named(lengths, turn):
        used = int((lengths > 0).sum())
        fixed = max(1, used // 4)
        passed = fixed + (places - fixed + turn * (used - fixed)) % max(1, number_of - fixed)
        return jnp.zeros((number_of,), jnp.int32).at[ranking[jnp.where(places < fixed, places, passed)]].set(jnp.asarray(lengths, jnp.int32))

    lengths = jnp.where(number % 4 == 0, named(heavy_load, number // 4), named(ordinary, number - number // 4 - 1))
    mixed = jax.random.permutation(jax.random.fold_in(own, 3), number_of)
    donor, receiver = mixed[0:number_of // 2 * 2:2], mixed[1:number_of // 2 * 2:2]
    margin = jnp.minimum(lengths[donor] - 1, reach - lengths[receiver]) // 2
    margin = jnp.where((donor == ranking[0]) | (receiver == ranking[0]) | (lengths[receiver] == 0), 0, jnp.maximum(margin, 0))
    passed = jax.random.randint(jax.random.fold_in(own, 4), (number_of // 2,), 0, 1 << 20) % (margin + 1)
    lengths = lengths.at[donor].add(-passed).at[receiver].add(passed)
    items = jnp.searchsorted(jnp.cumsum(lengths), jnp.arange(rows * top), side="right").astype(jnp.int32)
    grid = items.reshape(top, rows).T
    grid = grid[jax.random.permutation(jax.random.fold_in(own, 1), rows)]
    turn = jax.random.randint(jax.random.fold_in(own, 2), (rows, 1), 0, top)
    return jnp.take_along_axis(grid, (jnp.arange(top)[None, :] + turn) % top, axis=1)


def load_shares(count, total, bound, lean, full):
    weights = [(1 << 20) // math.isqrt(standing ** lean) + 1 for standing in range(1, count + 1)]
    largest = bound if full else min(bound, max(-(-total // count), total * weights[0] // sum(weights)))
    least = 1 if total - largest >= count - 1 else 0
    holding, surplus = [largest] + [least] * (count - 1), total - largest - least * (count - 1)
    while surplus > 0:
        candidates = [i for i in range(1, count) if holding[i] < largest] or [i for i in range(1, count) if holding[i] < bound]
        whole, remaining = sum([weights[i] for i in candidates]), surplus
        for i in candidates:
            extra = min(bound - holding[i], max(1, remaining * weights[i] // whole), surplus)
            holding[i] = holding[i] + extra
            surplus = surplus - extra
    return np.array(holding)


def centred(own_key, shape, deviation, bound, shards=(), kind=jnp.bfloat16):
    entries = jax.random.normal(own_key, shape, jnp.float32) * deviation
    if len(shards) > 0:
        entries = block_levels(own_key, shape, shards, -0.22, 0.18) * entries
    return jnp.clip(entries, min=-bound, max=bound).astype(kind)


def setup_inputs(seed: int = 0, part: int = 0) -> dict:
    arg_keys = jax.random.split(jax.random.key(seed), 20)
    own_keys = jax.random.split(jax.random.fold_in(arg_keys[19], part), 20)
    residual = centred(own_keys[0], (TOKENS, D), 1.0, 6.0, ((0, 16),))
    grouped_value_heads = centred(own_keys[1], (TOKENS, 2, GROUP_HEADS * HEAD_DIM), 1.0, 6.0, ((0, 4), (2, 4)))
    output_gate_heads = centred(own_keys[2], (TOKENS, 2, GROUP_HEADS * HEAD_DIM), 1.0, 6.0, ((0, 4), (2, 4)))
    projected_key_query = centred(own_keys[3], (TOKENS, 2 * STATE_ONE + 2 * STATE_TWO), 1.0, 6.0, ((0, 4),))
    raw_step_size = draw_raw_step_size(jax.random.fold_in(jax.random.fold_in(arg_keys[19], part), 71), part)
    step_size_bias = jnp.clip(-1.0 + 1.5 * jax.random.uniform(arg_keys[5], (2, GROUP_HEADS), jnp.float32) ** block_levels(arg_keys[5], (2, GROUP_HEADS), ((1, 4),), -0.2, 0.2), -1.0, 0.5)
    head_decay_logarithm = draw_head_decay_logarithm(jax.random.fold_in(arg_keys[19], 71), part)
    position_extra_decay = draw_position_extra_decay(jax.random.fold_in(jax.random.fold_in(arg_keys[19], part), 71), part)
    head_skip_weight = jnp.clip(0.5 + 1.5 * jax.random.uniform(arg_keys[8], (2, GROUP_HEADS), jnp.float32) ** block_levels(arg_keys[8], (2, GROUP_HEADS), ((1, 4),), -0.2, 0.2), 0.5, 2.0)
    value_kernel_taps = centred(arg_keys[9], (TAPS, 2, GROUP_HEADS * HEAD_DIM), 0.5, 3.0, ((2, 4),))
    key_query_kernel = centred(arg_keys[10], (TAPS, 2 * STATE_ONE + 2 * STATE_TWO), 0.5, 3.0)
    head_norm_gain = jnp.clip(1.0 + 0.18 * jax.random.normal(arg_keys[11], (2, GROUP_HEADS * HEAD_DIM), jnp.float32), 0.1, 1.9)
    output_matrix = centred(arg_keys[12], (2, GROUP_HEADS * HEAD_DIM, D), (2 * GROUP_HEADS * HEAD_DIM) ** -0.5, 0.125, ((1, 4),))
    expert_norm_gain = jnp.clip(1.0 + 0.18 * jax.random.normal(arg_keys[13], (D,), jnp.float32), 0.1, 1.9)
    expert_gate_weight = centred(arg_keys[14], (EXPERTS, D, FF), D ** -0.5, 0.125, ((0, 4), (2, 4)))
    expert_up_weight = centred(arg_keys[15], (EXPERTS, D, FF), D ** -0.5, 0.125, ((0, 4), (2, 4)))
    expert_down_weight = centred(arg_keys[16], (EXPERTS, FF, D), FF ** -0.5, 0.09375, ((0, 4), (1, 4)))
    token_expert_choice_keys = jax.random.split(jax.random.fold_in(own_keys[17], 1), TOKENS // ROWS_DEV)
    token_expert_choice_turns = jax.random.permutation(jax.random.fold_in(own_keys[17], 3), TOKENS // ROWS_DEV)
    token_expert_choice = jax.vmap(lambda own, number: deal_out(jax.random.fold_in(own_keys[17], 2), own, number, ROWS_DEV, EXPERTS, 2, CAP, 1))(token_expert_choice_keys, token_expert_choice_turns).reshape((TOKENS, 2))
    expert_output_weight = jnp.clip(0.2 + 0.8 * jax.random.uniform(own_keys[18], (TOKENS, 2), jnp.float32) ** block_levels(own_keys[18], (TOKENS, 2), ((0, 16),), -0.2, 0.2), 0.2, 1.0)
    return dict(residual=residual, grouped_value_heads=grouped_value_heads, output_gate_heads=output_gate_heads, projected_key_query=projected_key_query, raw_step_size=raw_step_size, step_size_bias=step_size_bias, head_decay_logarithm=head_decay_logarithm, position_extra_decay=position_extra_decay, head_skip_weight=head_skip_weight, value_kernel_taps=value_kernel_taps, key_query_kernel=key_query_kernel, head_norm_gain=head_norm_gain, output_matrix=output_matrix, expert_norm_gain=expert_norm_gain, expert_gate_weight=expert_gate_weight, expert_up_weight=expert_up_weight, expert_down_weight=expert_down_weight, token_expert_choice=token_expert_choice, expert_output_weight=expert_output_weight)


EPSILON = 1e-06

def causal_conv(signal, tap_weights):
    tap_count = tap_weights.shape[0]
    length = signal.shape[0]
    padded = jnp.pad(signal, ((tap_count - 1, 0), (0, 0)))
    summed = jnp.zeros((length, signal.shape[1]), jnp.float32)
    for offset in range(tap_count):
        summed = summed + padded[offset:offset + length].astype(jnp.float32) * tap_weights[offset].astype(jnp.float32)
    return summed

def advance(carried, pair_item):
    block_state, fading_step = pair_item
    return (carried * fading_step[:, None, None] + block_state, carried)

def group_scan(value_rows, key_rows, query_rows, step_spacing, decay_logarithm, block_size):
    positions, head_count, head_width = value_rows.shape
    block_count = positions // block_size
    value_rows = value_rows.reshape(block_count, block_size, head_count, head_width).astype(jnp.float32)
    key_rows = key_rows.reshape(block_count, block_size, key_rows.shape[-1]).astype(jnp.float32)
    query_rows = query_rows.reshape(block_count, block_size, query_rows.shape[-1]).astype(jnp.float32)
    step_spacing = step_spacing.reshape(block_count, block_size, head_count)
    running = jnp.cumsum(decay_logarithm.reshape(block_count, block_size, head_count), axis=1)
    scores = jnp.einsum('kln,ksn->kls', query_rows, key_rows)
    causal = jnp.tril(jnp.ones((block_size, block_size), jnp.bool_))
    spread = running[:, :, None, :] - running[:, None, :, :]
    damping = jnp.exp(jnp.where(causal[None, :, :, None], spread, -jnp.inf))
    weights = (scores[:, :, :, None] * damping * step_spacing[:, None, :, :]).astype(jnp.bfloat16)
    near_part = jnp.einsum('klsh,kshp->klhp', weights.astype(jnp.float32), value_rows)
    fading = jnp.exp(running[:, -1:, :] - running) * step_spacing
    scaled_keys = (key_rows[:, :, None, :] * fading[:, :, :, None]).astype(jnp.bfloat16)
    states = jnp.einsum('kshn,kshp->khpn', scaled_keys.astype(jnp.float32), value_rows)
    anchor = jnp.zeros(states.shape[1:], jnp.float32)
    last_state, entering = lax.scan(advance, anchor, (states, jnp.exp(running[:, -1, :])))
    far_part = jnp.einsum('kln,khpn->klhp', query_rows, entering, precision=lax.Precision.HIGHEST)
    far_part = far_part * jnp.exp(running)[:, :, :, None]
    return (near_part + far_part).reshape(positions, head_count, head_width)

def reference(residual, grouped_value_heads, output_gate_heads, projected_key_query, raw_step_size, step_size_bias, head_decay_logarithm, position_extra_decay, head_skip_weight, value_kernel_taps, key_query_kernel, head_norm_gain, output_matrix, expert_norm_gain, expert_gate_weight, expert_up_weight, expert_down_weight, token_expert_choice, expert_output_weight):
    lane_count = 2 * GROUP_HEADS * HEAD_DIM
    flat_values = grouped_value_heads.reshape(TOKENS, lane_count)
    conv_heads = jax.nn.silu(causal_conv(flat_values, value_kernel_taps.reshape(TAPS, lane_count))).astype(jnp.bfloat16)
    conv_rows = jax.nn.silu(causal_conv(projected_key_query, key_query_kernel)).astype(jnp.bfloat16)
    step_spacing = jax.nn.softplus(raw_step_size.astype(jnp.float32) + step_size_bias[None])
    decay_logarithm = position_extra_decay[:, None, None] - jnp.exp(head_decay_logarithm)[None] * step_spacing
    value_heads = conv_heads.reshape(TOKENS, 2, GROUP_HEADS, HEAD_DIM)
    bounds = [0, STATE_ONE, 2 * STATE_ONE, 2 * STATE_ONE + STATE_TWO, 2 * STATE_ONE + 2 * STATE_TWO]
    group_parts = []
    for group_index in range(2):
        key_rows = conv_rows[:, bounds[2 * group_index]:bounds[2 * group_index + 1]]
        query_rows = conv_rows[:, bounds[2 * group_index + 1]:bounds[2 * group_index + 2]]
        group_parts.append(group_scan(value_heads[:, group_index], key_rows, query_rows, step_spacing[:, group_index], decay_logarithm[:, group_index], BLOCK))
    mixer_sum = jnp.stack(group_parts, axis=1) + head_skip_weight[None, :, :, None] * value_heads.astype(jnp.float32)
    gated_rows = mixer_sum * jax.nn.silu(output_gate_heads.astype(jnp.float32).reshape(TOKENS, 2, GROUP_HEADS, HEAD_DIM))
    scale_rows = lax.rsqrt(lax.optimization_barrier(jnp.mean(gated_rows * gated_rows, axis=3, keepdims=True)) + EPSILON)
    mixed_heads = (gated_rows * scale_rows * head_norm_gain.reshape(2, GROUP_HEADS, HEAD_DIM)).astype(jnp.bfloat16)
    mix_out = jnp.dot(mixed_heads.reshape(TOKENS, lane_count), output_matrix.reshape(lane_count, D), preferred_element_type=jnp.float32)
    stream = (residual.astype(jnp.float32) + mix_out).astype(jnp.bfloat16)
    wide_stream = stream.astype(jnp.float32)
    normed = (wide_stream * lax.rsqrt(lax.optimization_barrier(jnp.mean(wide_stream * wide_stream, axis=1, keepdims=True)) + EPSILON) * expert_norm_gain[None]).astype(jnp.bfloat16)
    sources = TOKENS // ROWS_DEV
    flat_ids = token_expert_choice.reshape(sources, 2 * ROWS_DEV)
    matches = (flat_ids[:, :, None] == jnp.arange(EXPERTS, dtype=jnp.int32)[None, None, :]).astype(jnp.int32)
    slot_rank = lax.optimization_barrier(jnp.sum((jnp.cumsum(matches, axis=1) - matches) * matches, axis=2))
    column = jnp.arange(sources, dtype=jnp.int32)[:, None] * CAP + slot_rank
    token_index = jnp.repeat(jnp.arange(TOKENS, dtype=jnp.int32).reshape(sources, ROWS_DEV), 2, axis=1)
    slot_table = jnp.zeros((EXPERTS, sources * CAP), jnp.int32).at[flat_ids.reshape(-1), column.reshape(-1)].set(token_index.reshape(-1))
    slice_width = FF // N_TP

    def one_expert(expert_index):
        gathered = jnp.take(normed, slot_table[expert_index], axis=0)
        gate_out = jnp.dot(gathered, expert_gate_weight[expert_index], preferred_element_type=jnp.float32)
        up_out = jnp.dot(gathered, expert_up_weight[expert_index], preferred_element_type=jnp.float32)
        hidden = (jax.nn.silu(gate_out) * up_out).astype(jnp.bfloat16)
        sliced = hidden.reshape(gathered.shape[0], N_TP, slice_width).astype(jnp.float32)
        down_slices = expert_down_weight[expert_index].reshape(N_TP, slice_width, D).astype(jnp.float32)
        pieces = jnp.einsum('rtf,tfd->rtd', sliced, down_slices).astype(jnp.bfloat16)
        pieces = lax.optimization_barrier(pieces).astype(jnp.float32)
        return lax.optimization_barrier(jnp.sum(pieces, axis=1)).astype(jnp.bfloat16)
    outputs = lax.map(one_expert, jnp.arange(EXPERTS, dtype=jnp.int32))
    picked = outputs[flat_ids.reshape(-1), column.reshape(-1)].reshape(TOKENS, 2, D).astype(jnp.float32)
    weighted = expert_output_weight[:, 0:1] * picked[:, 0] + expert_output_weight[:, 1:2] * picked[:, 1]
    return (wide_stream + weighted).astype(jnp.bfloat16)
```

```python
import jax
import jax.numpy as jnp
from jax import lax
from jax.sharding import PartitionSpec as P

HEAD_DIM = 64
STATE_ONE = 64
STATE_TWO = 128
BLOCK = 128


EPSILON = 1e-06


def passed_along(shard, axis, by):
    length = lax.axis_size(axis)
    pairs = [(i, i + by) for i in range(length) if 0 <= i + by < length]
    return lax.ppermute(shard, axis, pairs)


def prefix(shard, axis, join, neutral):
    place = lax.axis_index(axis)
    gathered = jax.tree.map(
        lambda a, kind: lax.all_gather(a.astype(kind), axis),
        shard,
        (jnp.bfloat16, jnp.bfloat16, jnp.bfloat16),
    )
    state = jax.tree.map(lambda a, e: jnp.zeros_like(a) + jnp.asarray(e, a.dtype), shard, neutral)

    def one(step, state):
        return join(
            state,
            jax.tree.map(
                lambda a, own: lax.dynamic_index_in_dim(a, step, 0, False).astype(own.dtype),
                gathered,
                shard,
            ),
        )

    return lax.fori_loop(0, place, one, state)


def causal_taps(extended, tap_weights, length):
    summed = jnp.zeros((length, extended.shape[1]), jnp.float32)
    for offset in range(tap_weights.shape[0]):
        summed = summed + extended[offset : offset + length].astype(jnp.float32) * tap_weights[
            offset
        ].astype(jnp.float32)
    return summed


def advance(carried, pair_item):
    block_state, fading_step = pair_item
    return (carried * fading_step[:, None, None] + block_state, carried)


def local_blocks(value_rows, key_rows, query_rows, step_spacing, decay_logarithm):
    positions, head_count, head_width = value_rows.shape
    block_count = positions // BLOCK
    value_rows = value_rows.reshape(block_count, BLOCK, head_count, head_width)
    key_rows = key_rows.reshape(block_count, BLOCK, key_rows.shape[-1])
    query_rows = query_rows.reshape(block_count, BLOCK, query_rows.shape[-1])
    step_spacing = step_spacing.reshape(block_count, BLOCK, head_count)
    running = jnp.cumsum(decay_logarithm.reshape(block_count, BLOCK, head_count), axis=1)
    scores = jnp.einsum("kln,ksn->kls", query_rows, key_rows, preferred_element_type=jnp.float32)
    causal = jnp.tril(jnp.ones((BLOCK, BLOCK), jnp.bool_))
    spread = running[:, :, None, :] - running[:, None, :, :]
    damping = jnp.exp(jnp.where(causal[None, :, :, None], spread, -jnp.inf))
    weights = (scores[:, :, :, None] * damping * step_spacing[:, None, :, :]).astype(jnp.bfloat16)
    near_part = jnp.einsum(
        "klsh,kshp->klhp", weights, value_rows, preferred_element_type=jnp.float32
    )
    fading = jnp.exp(running[:, -1:, :] - running) * step_spacing
    scaled_keys = (key_rows.astype(jnp.float32)[:, :, None, :] * fading[:, :, :, None]).astype(
        jnp.bfloat16
    )
    states = jnp.einsum(
        "kshn,kshp->khpn", scaled_keys, value_rows, preferred_element_type=jnp.float32
    )
    block_ends = running[:, -1, :]
    anchor = jnp.zeros(states.shape[1:], jnp.float32)
    last_state, entering = lax.scan(advance, anchor, (states, jnp.exp(block_ends)))
    wide_queries = query_rows.astype(jnp.float32)
    far_part = jnp.einsum("kln,khpn->klhp", wide_queries, entering, precision=lax.Precision.HIGHEST)
    far_part = far_part * jnp.exp(running)[:, :, :, None]
    earlier_ends = jnp.cumsum(block_ends, axis=0) - block_ends
    carried_decay = jnp.exp(running + earlier_ends[:, None, :])
    return (
        near_part + far_part,
        last_state,
        jnp.sum(block_ends, axis=0),
        wide_queries,
        carried_decay,
    )


def join_states(earlier, later):
    early_decay, early_one, early_two = earlier
    late_decay, late_one, late_two = later
    return (
        early_decay + late_decay,
        early_one * jnp.exp(late_decay[0])[:, None, None] + late_one,
        early_two * jnp.exp(late_decay[1])[:, None, None] + late_two,
    )


def routed_experts(
    wide_stream, normed, gate_weight, up_weight, down_weight, token_expert_choice, expert_output_weight
):
    rows_here, model_width = normed.shape
    expert_total = lax.axis_size("sp")
    capacity = 2 * rows_here // expert_total + 1
    flat_ids = token_expert_choice.reshape(-1)
    matches = (flat_ids[:, None] == jnp.arange(expert_total, dtype=jnp.int32)[None, :]).astype(
        jnp.int32
    )
    slot_rank = jnp.sum((jnp.cumsum(matches, axis=0) - matches) * matches, axis=1)
    target = flat_ids * capacity + slot_rank
    outbound = (
        jnp.zeros((expert_total * capacity, model_width), jnp.bfloat16)
        .at[target]
        .set(jnp.repeat(normed, 2, axis=0))
    )
    outbound = outbound.reshape(expert_total, capacity, model_width)
    widened = lax.all_gather(
        lax.all_to_all(outbound, "sp", split_axis=0, concat_axis=0, tiled=True),
        "tp",
        axis=0,
        tiled=True,
    )
    flat_rows = widened.reshape(-1, widened.shape[-1])
    gate_out = jnp.dot(flat_rows, gate_weight, preferred_element_type=jnp.float32)
    up_out = jnp.dot(flat_rows, up_weight, preferred_element_type=jnp.float32)
    hidden = (jax.nn.silu(gate_out) * up_out).astype(jnp.bfloat16)
    partial_value = jnp.dot(
        hidden, down_weight, preferred_element_type=jnp.float32
    ).astype(jnp.bfloat16)
    partial_value = lax.optimization_barrier(
        partial_value.reshape(widened.shape[0], widened.shape[1], partial_value.shape[-1])
    ).astype(jnp.float32)
    summed = lax.psum_scatter(
        partial_value.astype(jnp.bfloat16), "tp", scatter_dimension=0, tiled=True
    )
    returned = lax.all_to_all(summed, "sp", split_axis=0, concat_axis=0, tiled=True)
    picked = jnp.take(returned.reshape(expert_total * capacity, model_width), target, axis=0)
    picked = picked.reshape(rows_here, 2, model_width).astype(jnp.float32)
    weighted = (
        expert_output_weight[:, 0:1] * picked[:, 0] + expert_output_weight[:, 1:2] * picked[:, 1]
    )
    return (wide_stream + weighted).astype(jnp.bfloat16)


def arrival_order(place, length):
    order = []
    for hops in range(1, length):
        if place - hops >= 0:
            order.append((hops, True))
        if place + hops < length:
            order.append((hops, False))
    return order


def select_by_place(place, choices):
    distinct = []
    for array in choices:
        if not any(array is d for d in distinct):
            distinct.append(array)
    out = distinct[0]
    for array in distinct[1:]:
        here = jnp.zeros((), jnp.bool_)
        for i, c in enumerate(choices):
            if c is array:
                here = here | (place == i)
        out = jnp.where(here, array, out)
    return out


def line_blocks(block, axis):
    length = lax.axis_size(axis)
    place = lax.axis_index(axis)
    from_left, from_right = [block], [block]
    for hops in range(1, length):
        rightward = [(i, i + 1) for i in range(hops - 1, length - 1)]
        leftward = [(length - 1 - i, length - 2 - i) for i in range(hops - 1, length - 1)]
        from_left.append(lax.ppermute(from_left[-1], axis, rightward))
        from_right.append(lax.ppermute(from_right[-1], axis, leftward))
    orders = [arrival_order(i, length) for i in range(length)]
    arrived = [block]
    for turn in range(length - 1):
        arrived.append(
            select_by_place(
                place,
                [
                    (from_left if orders[i][turn][1] else from_right)[orders[i][turn][0]]
                    for i in range(length)
                ],
            )
        )
    return arrived


def source_table(length):
    table = []
    for i in range(length):
        table.append(
            [i] + [i - hops if left else i + hops for hops, left in arrival_order(i, length)]
        )
    return table


def line_reduce(parts, axis):
    length = lax.axis_size(axis)
    place = lax.axis_index(axis)
    turn_of = [{d: t for t, d in enumerate(row)} for row in source_table(length)]

    def added(block, received):
        if received is None:
            return block
        return (block.astype(jnp.float32) + received.astype(jnp.float32)).astype(block.dtype)

    right, left = None, None
    for step in range(1, length):
        goes_right = [parts[turn_of[i][min(length - step + i, length - 1)]] for i in range(length)]
        goes_left = [parts[turn_of[i][max(step - length + i, 0)]] for i in range(length)]
        for i in range(step, length):
            goes_right[i] = goes_right[step - 1]
        for i in range(length - step):
            goes_left[i] = goes_left[length - step]
        right = lax.ppermute(
            added(select_by_place(place, goes_right), right),
            axis,
            [(i, i + 1) for i in range(min(step, length - 1))],
        )
        left = lax.ppermute(
            added(select_by_place(place, goes_left), left),
            axis,
            [(length - 1 - i, length - 2 - i) for i in range(min(step, length - 1))],
        )
    return parts[0].astype(jnp.float32) + right.astype(jnp.float32) + left.astype(jnp.float32)


def swapped(array, bit):
    return lax.ppermute(array, "sp", [(i, i ^ bit) for i in range(lax.axis_size("sp"))])


def dense_experts(
    wide_stream, normed, gate_weight, up_weight, down_weight, token_expert_choice, expert_output_weight
):
    rows_here, model_width = normed.shape
    expert_total = lax.axis_size("sp")
    length = lax.axis_size("tp")
    place = lax.axis_index("tp")
    mine = lax.axis_index("sp")
    capacity = 2 * rows_here // expert_total + 1
    slots = -(-4 * capacity // 8) * 8
    facts = jnp.concatenate(
        [token_expert_choice.astype(jnp.float32), expert_output_weight], axis=1
    ).T
    facts = lax.all_gather(lax.all_gather(facts, "tp"), "sp")
    blocks = line_blocks(normed, "tp")
    across = [swapped(b, 2) for b in blocks]
    sources = jnp.asarray(source_table(length), jnp.int32)[place]
    sums = []
    for turn in range(length):
        pair = [blocks[turn], across[turn]]
        four = [pair[0], swapped(pair[0], 1), pair[1], swapped(pair[1], 1)]
        rows = jnp.concatenate(four, axis=0)
        known = jnp.stack(
            [facts[mine ^ bit, sources[turn]] for bit in (0, 1, 2, 3)], axis=1
        ).reshape(4, 4 * rows_here)
        named = known[:2] == mine.astype(jnp.float32)
        weight = jnp.sum(jnp.where(named, known[2:], 0.0), axis=0)
        here = jnp.any(named, axis=0)
        rank = jnp.cumsum(here.astype(jnp.int32)) - 1
        slot = jnp.where(here, rank, -1)
        chosen = (jnp.arange(slots, dtype=jnp.int32)[:, None] == slot[None, :]).astype(jnp.bfloat16)
        taken = jnp.dot(chosen, rows, preferred_element_type=jnp.float32).astype(jnp.bfloat16)
        gate_out = jnp.dot(taken, gate_weight, preferred_element_type=jnp.float32)
        up_out = jnp.dot(taken, up_weight, preferred_element_type=jnp.float32)
        hidden = (jax.nn.silu(gate_out) * up_out).astype(jnp.bfloat16)
        result = jnp.dot(hidden, down_weight, preferred_element_type=jnp.float32).astype(
            jnp.bfloat16
        )
        spread = lax.dot_general(
            chosen, result, (((0,), (0,)), ((), ())), preferred_element_type=jnp.float32
        )
        sums.append((spread * weight[:, None]).astype(jnp.bfloat16).reshape(4, rows_here, model_width))

    def added(one, two):
        return (one.astype(jnp.float32) + two.astype(jnp.float32)).astype(jnp.bfloat16)

    parts = [None] * length
    for turn in reversed(range(length)):
        near = added(sums[turn][0], swapped(sums[turn][1], 1))
        far = added(sums[turn][2], swapped(sums[turn][3], 1))
        parts[turn] = added(near, swapped(far, 2))
    return (wide_stream + line_reduce(parts, "tp")).astype(jnp.bfloat16)


def local(
    residual,
    grouped_value_heads,
    output_gate_heads,
    projected_key_query,
    raw_step_size,
    step_size_bias,
    head_decay_logarithm,
    position_extra_decay,
    head_skip_weight,
    value_kernel_taps,
    key_query_kernel,
    head_norm_gain,
    output_matrix,
    expert_norm_gain,
    expert_gate_weight,
    expert_up_weight,
    expert_down_weight,
    token_expert_choice,
    expert_output_weight,
):
    positions = grouped_value_heads.shape[0]
    lane_width = grouped_value_heads.shape[2]
    local_heads = lane_width // HEAD_DIM
    both_lanes = 2 * lane_width
    rim_depth = key_query_kernel.shape[0] - 1
    flat_values = grouped_value_heads.reshape(positions, both_lanes)
    rim_rows = jnp.concatenate(
        [flat_values[positions - rim_depth :], projected_key_query[positions - rim_depth :]], axis=1
    )
    prior_rows = passed_along(rim_rows, "sp", 1)
    padded_values = jnp.concatenate([prior_rows[:, :both_lanes], flat_values], axis=0)
    padded_keys = jnp.concatenate([prior_rows[:, both_lanes:], projected_key_query], axis=0)
    conv_heads = jax.nn.silu(
        causal_taps(padded_values, value_kernel_taps.reshape(rim_depth + 1, both_lanes), positions)
    ).astype(jnp.bfloat16)
    conv_rows = jax.nn.silu(causal_taps(padded_keys, key_query_kernel, positions)).astype(
        jnp.bfloat16
    )
    step_spacing = jax.nn.softplus(raw_step_size.astype(jnp.float32) + step_size_bias[None])
    decay_logarithm = (
        position_extra_decay[:, None, None] - jnp.exp(head_decay_logarithm)[None] * step_spacing
    )
    value_heads = conv_heads.reshape(positions, 2, local_heads, HEAD_DIM)
    bounds = [0, STATE_ONE, 2 * STATE_ONE, 2 * STATE_ONE + STATE_TWO, 2 * STATE_ONE + 2 * STATE_TWO]
    local_parts = []
    end_states = []
    decay_totals = []
    query_list = []
    reach_list = []
    for group_index in range(2):
        key_rows = conv_rows[:, bounds[2 * group_index] : bounds[2 * group_index + 1]]
        query_rows = conv_rows[:, bounds[2 * group_index + 1] : bounds[2 * group_index + 2]]
        local_part, end_state, decay_total, wide_queries, carried_decay = local_blocks(
            value_heads[:, group_index],
            key_rows,
            query_rows,
            step_spacing[:, group_index],
            decay_logarithm[:, group_index],
        )
        local_parts.append(local_part)
        end_states.append(end_state)
        decay_totals.append(decay_total)
        query_list.append(wide_queries)
        reach_list.append(carried_decay)
    identity = (
        jnp.zeros((2, local_heads), jnp.float32),
        jnp.zeros_like(end_states[0]),
        jnp.zeros_like(end_states[1]),
    )
    prior_decay, enter_one, enter_two = prefix(
        (jnp.stack(decay_totals), end_states[0], end_states[1]), "sp", join_states, identity
    )
    entered = [enter_one, enter_two]
    group_parts = []
    for group_index in range(2):
        carried_part = jnp.einsum(
            "kln,hpn->klhp",
            query_list[group_index],
            entered[group_index],
            precision=lax.Precision.HIGHEST,
        )
        carried_part = carried_part * reach_list[group_index][:, :, :, None]
        summed_part = local_parts[group_index] + carried_part
        group_parts.append(summed_part.reshape(positions, local_heads, HEAD_DIM))
    mixer_sum = jnp.stack(group_parts, axis=1) + head_skip_weight[
        None, :, :, None
    ] * value_heads.astype(jnp.float32)
    gated_rows = mixer_sum * jax.nn.silu(
        output_gate_heads.astype(jnp.float32).reshape(positions, 2, local_heads, HEAD_DIM)
    )
    scale_rows = lax.rsqrt(jnp.mean(gated_rows * gated_rows, axis=3, keepdims=True) + EPSILON)
    mixed_heads = (
        gated_rows * scale_rows * head_norm_gain.reshape(2, local_heads, HEAD_DIM)
    ).astype(jnp.bfloat16)
    mixed_heads = mixed_heads.reshape(positions, 2, lane_width)
    rows_here = residual.shape[0]
    model_width = output_matrix.shape[2]
    mix_out = lax.psum_scatter(
        jnp.einsum(
            "tgc,gcd->td", mixed_heads, output_matrix, preferred_element_type=jnp.float32
        ).astype(jnp.bfloat16),
        "tp",
        scatter_dimension=0,
        tiled=True,
    ).astype(jnp.float32)
    stream = (residual.astype(jnp.float32) + mix_out).astype(jnp.bfloat16)
    wide_stream = stream.astype(jnp.float32)
    normed = (
        wide_stream
        * lax.rsqrt(jnp.mean(wide_stream * wide_stream, axis=1, keepdims=True) + EPSILON)
        * expert_norm_gain[None]
    ).astype(jnp.bfloat16)
    operands = (
        wide_stream,
        normed,
        expert_gate_weight[0],
        expert_up_weight[0],
        expert_down_weight[0],
        token_expert_choice,
        expert_output_weight,
    )
    if lax.axis_size("sp") == 4:
        return dense_experts(*operands)
    return routed_experts(*operands)


def solution(mesh):
    placed = (
        P(("grp", "sp", "tp"), None),
        P(("grp", "sp"), None, "tp"),
        P(("grp", "sp"), None, "tp"),
        P(("grp", "sp"), None),
        P(("grp", "sp"), None, "tp"),
        P(None, "tp"),
        P(None, "tp"),
        P(("grp", "sp")),
        P(None, "tp"),
        P(None, None, "tp"),
        P(),
        P(None, "tp"),
        P(None, "tp", None),
        P(),
        P("sp", None, "tp"),
        P("sp", None, "tp"),
        P("sp", "tp", None),
        P(("grp", "sp", "tp"), None),
        P(("grp", "sp", "tp"), None),
    )
    return jax.shard_map(
        local, mesh=mesh, in_specs=placed, out_specs=P(("grp", "sp", "tp"), None), check_vma=False
    )
```

```python
import functools

import jax
import jax.numpy as jnp
from jax import lax
from jax.experimental import pallas as pl
from jax.experimental.pallas import tpu as pltpu
from jax.sharding import PartitionSpec as P

HEAD_DIM = 64
STATE_ONE = 64
STATE_TWO = 128
BLOCK = 128


EPSILON = 1e-06


def passed_along(shard, axis, by):
    length = lax.axis_size(axis)
    pairs = [(i, i + by) for i in range(length) if 0 <= i + by < length]
    return lax.ppermute(shard, axis, pairs)


def high_rows(heads):
    return -(-2 * heads // 8) * 8


def widened(column, heads, width):
    rows = column.shape[0]
    return jnp.concatenate(
        [jnp.broadcast_to(column[:, h : h + 1], (rows, width)) for h in range(heads)], axis=1
    )


def spread_down(tall, first, heads, width):
    return jnp.concatenate(
        [jnp.broadcast_to(tall[first + h : first + h + 1], (1, width)) for h in range(heads)], axis=1
    )


def both_groups(tall, heads, width):
    return jnp.concatenate(
        [spread_down(tall, g * heads, heads, width) for g in range(2)], axis=1
    )


def states_kernel(
    heads,
    sizes,
    values_ref,
    keys_ref,
    rim_ref,
    value_taps_ref,
    key_taps_ref,
    steps_ref,
    facts_ref,
    extra_ref,
    x_ref,
    rows_ref,
    across_ref,
    down_ref,
    enter_one_ref,
    enter_two_ref,
    earlier_ref,
    packed_ref,
    tail_ref,
    one_ref,
    two_ref,
    sum_ref,
):
    step = pl.program_id(0)
    lanes = heads * HEAD_DIM
    taps = value_taps_ref.shape[0]

    @pl.when(step == 0)
    def _():
        tail_ref[...] = rim_ref[...].astype(jnp.float32)
        one_ref[...] = jnp.zeros_like(one_ref)
        two_ref[...] = jnp.zeros_like(two_ref)
        sum_ref[...] = jnp.zeros_like(sum_ref)

    here = jnp.concatenate(
        [values_ref[...].astype(jnp.float32), keys_ref[...].astype(jnp.float32)], axis=1
    )
    extended = jnp.concatenate([tail_ref[...], here], axis=0)
    tail_ref[...] = here[BLOCK - 8 :]
    weights = jnp.concatenate(
        [value_taps_ref[...].astype(jnp.float32), key_taps_ref[...].astype(jnp.float32)], axis=1
    )
    summed = jnp.zeros_like(here)
    for j in range(taps):
        first = 8 - (taps - 1) + j
        summed = summed + extended[first : first + BLOCK] * weights[j : j + 1]
    active = (summed * jax.nn.sigmoid(summed)).astype(jnp.bfloat16)
    x = active[:, : 2 * lanes]
    rows = active[:, 2 * lanes :]
    x_ref[...] = x
    rows_ref[...] = rows

    raw = steps_ref[...] + facts_ref[:, 0:1]
    stride = jnp.maximum(raw, 0.0) + jnp.log1p(jnp.exp(-jnp.abs(raw)))
    log_decay = extra_ref[...] - jnp.exp(facts_ref[:, 1:2]) * stride
    upto = (
        lax.broadcasted_iota(jnp.int32, (BLOCK, BLOCK), 0)
        <= lax.broadcasted_iota(jnp.int32, (BLOCK, BLOCK), 1)
    ).astype(jnp.float32)
    running = jnp.dot(
        log_decay, upto, preferred_element_type=jnp.float32, precision=lax.Precision.HIGHEST
    )
    end = running[:, BLOCK - 1 :]
    fading = jnp.exp(end - running) * stride
    high = running.shape[0]
    stacked = jnp.concatenate(
        [running, fading, jnp.exp(running)]
        + [jnp.zeros((BLOCK - 3 * high, BLOCK), jnp.float32)],
        axis=0,
    )
    down = stacked.T
    across_ref[...] = jnp.concatenate([running, stride], axis=0)
    down_ref[...] = down
    earlier_ref[...] = jnp.broadcast_to(
        jnp.exp(both_groups(sum_ref[...], heads, HEAD_DIM)), earlier_ref.shape
    )
    faded_end = jnp.exp(both_groups(end, heads, HEAD_DIM))
    bound = 0
    for g, (enter_ref, state_ref) in enumerate(((enter_one_ref, one_ref), (enter_two_ref, two_ref))):
        keys = rows[:, bound : bound + sizes[g]]
        bound += 2 * sizes[g]
        fade = widened(down[:, high + g * heads : high + (g + 1) * heads], heads, HEAD_DIM)
        scaled = (x[:, g * lanes : (g + 1) * lanes].astype(jnp.float32) * fade).astype(jnp.bfloat16)
        own = lax.dot_general(
            keys, scaled, (((0,), (0,)), ((), ())), preferred_element_type=jnp.float32
        )
        state = state_ref[...]
        enter_ref[0] = state
        state_ref[...] = state * faded_end[:, g * lanes : (g + 1) * lanes] + own
    total = sum_ref[...] + end
    sum_ref[...] = total

    @pl.when(step == pl.num_programs(0) - 1)
    def _():
        whole = both_groups(total, heads, HEAD_DIM)
        high_part = whole.astype(jnp.bfloat16)
        low_part = (whole - high_part.astype(jnp.float32)).astype(jnp.bfloat16)
        packed_ref[0 : sizes[0]] = one_ref[...].astype(jnp.bfloat16)
        packed_ref[sizes[0] : sizes[0] + sizes[1]] = two_ref[...].astype(jnp.bfloat16)
        packed_ref[sizes[0] + sizes[1] :] = jnp.concatenate(
            [
                jnp.broadcast_to(part[:, g * lanes : (g + 1) * lanes].astype(jnp.float32), (4, lanes))
                for g in range(2)
                for part in (high_part, low_part)
            ],
            axis=0,
        ).astype(jnp.bfloat16)


def near_kernel(heads, sizes, x_ref, rows_ref, across_ref, down_ref, facts_ref, near_ref):
    lanes = heads * HEAD_DIM
    high = across_ref.shape[0] // 2
    later = lax.broadcasted_iota(jnp.int32, (BLOCK, BLOCK), 0) >= lax.broadcasted_iota(
        jnp.int32, (BLOCK, BLOCK), 1
    )
    skip = both_groups(facts_ref[:, 2:3], heads, HEAD_DIM)
    bound = 0
    out = []
    for g in range(2):
        keys = rows_ref[:, bound : bound + sizes[g]]
        queries = rows_ref[:, bound + sizes[g] : bound + 2 * sizes[g]]
        bound += 2 * sizes[g]
        scores = lax.dot_general(
            queries, keys, (((1,), (1,)), ((), ())), preferred_element_type=jnp.float32
        )
        for h in range(heads):
            i = g * heads + h
            spread = jnp.where(later, down_ref[:, i : i + 1] - across_ref[i : i + 1], -1e30)
            weights = scores * jnp.exp(spread) * across_ref[high + i : high + i + 1]
            x = x_ref[:, i * HEAD_DIM : (i + 1) * HEAD_DIM]
            out.append(
                jnp.dot(weights.astype(jnp.bfloat16), x, preferred_element_type=jnp.float32)
            )
    near_ref[...] = jnp.concatenate(out, axis=1) + skip * x_ref[...].astype(jnp.float32)


def mixed_kernel(heads, sizes, prior_count, *refs):
    priors = refs[:prior_count]
    (
        near_ref,
        rows_ref,
        down_ref,
        enter_one_ref,
        enter_two_ref,
        earlier_ref,
        gate_ref,
        gain_ref,
        out_ref,
        one_ref,
        two_ref,
    ) = refs[prior_count:]
    lanes = heads * HEAD_DIM
    high = high_rows(heads)

    @pl.when(pl.program_id(0) == 0)
    def _():
        base = sizes[0] + sizes[1]
        for g, state_ref in enumerate((one_ref, two_ref)):
            state = jnp.zeros_like(state_ref)
            first = g * sizes[0]
            for prior in reversed(priors):
                facts = prior[base:].astype(jnp.float32)
                decay = facts[8 * g : 8 * g + 1] + facts[8 * g + 4 : 8 * g + 5]
                own = prior[first : first + sizes[g]].astype(jnp.float32)
                state = state * jnp.exp(decay) + own
            state_ref[...] = state

    bound = 0
    for g, (enter_ref, state_ref) in enumerate(((enter_one_ref, one_ref), (enter_two_ref, two_ref))):
        queries = rows_ref[:, bound + sizes[g] : bound + 2 * sizes[g]]
        bound += 2 * sizes[g]
        here = slice(g * lanes, (g + 1) * lanes)
        entering = enter_ref[0] + state_ref[...] * earlier_ref[0:1, here]
        far = jnp.dot(
            queries, entering.astype(jnp.bfloat16), preferred_element_type=jnp.float32
        )
        reach = down_ref[:, 2 * high + g * heads : 2 * high + (g + 1) * heads]
        gate = gate_ref[:, here].astype(jnp.float32)
        total = near_ref[:, here] + far * widened(reach, heads, HEAD_DIM)
        gated = total * (gate * jax.nn.sigmoid(gate))
        squares = gated * gated
        means = jnp.concatenate(
            [
                jnp.sum(squares[:, h * HEAD_DIM : (h + 1) * HEAD_DIM], axis=1, keepdims=True)
                for h in range(heads)
            ],
            axis=1,
        ) * (1.0 / HEAD_DIM)
        scale = widened(lax.rsqrt(means + EPSILON), heads, HEAD_DIM)
        out_ref[:, here] = (gated * scale * gain_ref[:, here]).astype(jnp.bfloat16)


def mixed_rows(
    grouped_value_heads,
    output_gate_heads,
    projected_key_query,
    raw_step_size,
    step_size_bias,
    head_decay_logarithm,
    position_extra_decay,
    head_skip_weight,
    value_kernel_taps,
    key_query_kernel,
    head_norm_gain,
):
    positions, _, lanes = grouped_value_heads.shape
    heads = lanes // HEAD_DIM
    high = high_rows(heads)
    sizes = (STATE_ONE, STATE_TWO)
    width = key_query_kernel.shape[1]
    blocks = positions // BLOCK
    last = grouped_value_heads[positions - 8 :].reshape(8, 2 * lanes)
    rim = passed_along(
        jnp.concatenate([last, projected_key_query[positions - 8 :]], axis=1), "sp", 1
    )
    values = grouped_value_heads.reshape(positions, 2 * lanes)
    facts = jnp.stack(
        [step_size_bias.reshape(-1), head_decay_logarithm.reshape(-1), head_skip_weight.reshape(-1)],
        axis=1,
    )
    facts = jnp.pad(facts, ((0, high - 2 * heads), (0, 0)))
    steps = raw_step_size.reshape(positions, 2 * heads).T.astype(jnp.float32)
    steps = jnp.pad(steps, ((0, high - 2 * heads), (0, 0)))

    def by_block(rows, columns):
        return pl.BlockSpec((rows, columns), lambda k: (k, 0))

    def along(rows):
        return pl.BlockSpec((rows, BLOCK), lambda k: (0, k))

    def fixed(*shape):
        return pl.BlockSpec(shape, lambda k: (0,) * len(shape))

    def per_block(*shape):
        return pl.BlockSpec((1, *shape), lambda k: (k,) + (0,) * len(shape))

    f32, bf16 = jnp.float32, jnp.bfloat16
    packed_rows = sizes[0] + sizes[1] + 16
    x, rows, across, down, enter_one, enter_two, earlier, packed = pl.pallas_call(
        functools.partial(states_kernel, heads, sizes),
        grid=(blocks,),
        in_specs=[
            by_block(BLOCK, 2 * lanes),
            by_block(BLOCK, width),
            fixed(8, 2 * lanes + width),
            fixed(value_kernel_taps.shape[0], 2 * lanes),
            fixed(*key_query_kernel.shape),
            along(high),
            fixed(high, 3),
            along(1),
        ],
        out_specs=[
            by_block(BLOCK, 2 * lanes),
            by_block(BLOCK, width),
            along(2 * high),
            by_block(BLOCK, BLOCK),
            per_block(sizes[0], lanes),
            per_block(sizes[1], lanes),
            by_block(8, 2 * lanes),
            fixed(packed_rows, lanes),
        ],
        out_shape=[
            jax.ShapeDtypeStruct((positions, 2 * lanes), bf16),
            jax.ShapeDtypeStruct((positions, width), bf16),
            jax.ShapeDtypeStruct((2 * high, positions), f32),
            jax.ShapeDtypeStruct((positions, BLOCK), f32),
            jax.ShapeDtypeStruct((blocks, sizes[0], lanes), f32),
            jax.ShapeDtypeStruct((blocks, sizes[1], lanes), f32),
            jax.ShapeDtypeStruct((8 * blocks, 2 * lanes), f32),
            jax.ShapeDtypeStruct((packed_rows, lanes), bf16),
        ],
        scratch_shapes=[
            pltpu.VMEM((8, 2 * lanes + width), f32),
            pltpu.VMEM((sizes[0], lanes), f32),
            pltpu.VMEM((sizes[1], lanes), f32),
            pltpu.VMEM((high, 1), f32),
        ],
        name="states",
    )(
        values,
        projected_key_query,
        rim,
        value_kernel_taps.reshape(-1, 2 * lanes),
        key_query_kernel,
        steps,
        facts,
        position_extra_decay[None],
    )
    priors = [passed_along(packed, "sp", by) for by in range(1, lax.axis_size("sp"))]
    near = pl.pallas_call(
        functools.partial(near_kernel, heads, sizes),
        grid=(blocks,),
        in_specs=[
            by_block(BLOCK, 2 * lanes),
            by_block(BLOCK, width),
            along(2 * high),
            by_block(BLOCK, BLOCK),
            fixed(high, 3),
        ],
        out_specs=by_block(BLOCK, 2 * lanes),
        out_shape=jax.ShapeDtypeStruct((positions, 2 * lanes), f32),
        name="near",
    )(x, rows, across, down, facts)
    return pl.pallas_call(
        functools.partial(mixed_kernel, heads, sizes, len(priors)),
        grid=(blocks,),
        in_specs=[fixed(packed_rows, lanes) for _ in priors]
        + [
            by_block(BLOCK, 2 * lanes),
            by_block(BLOCK, width),
            by_block(BLOCK, BLOCK),
            per_block(sizes[0], lanes),
            per_block(sizes[1], lanes),
            by_block(8, 2 * lanes),
            by_block(BLOCK, 2 * lanes),
            fixed(1, 2 * lanes),
        ],
        out_specs=by_block(BLOCK, 2 * lanes),
        out_shape=jax.ShapeDtypeStruct((positions, 2 * lanes), bf16),
        scratch_shapes=[
            pltpu.VMEM((sizes[0], lanes), f32),
            pltpu.VMEM((sizes[1], lanes), f32),
        ],
        name="mixed",
    )(
        *priors,
        near,
        rows,
        down,
        enter_one,
        enter_two,
        earlier,
        output_gate_heads.reshape(positions, 2 * lanes),
        head_norm_gain.reshape(1, 2 * lanes),
    )


def routed_experts(
    wide_stream, normed, gate_weight, up_weight, down_weight, token_expert_choice, expert_output_weight
):
    rows_here, model_width = normed.shape
    expert_total = lax.axis_size("sp")
    capacity = 2 * rows_here // expert_total + 1
    flat_ids = token_expert_choice.reshape(-1)
    matches = (flat_ids[:, None] == jnp.arange(expert_total, dtype=jnp.int32)[None, :]).astype(
        jnp.int32
    )
    slot_rank = jnp.sum((jnp.cumsum(matches, axis=0) - matches) * matches, axis=1)
    target = flat_ids * capacity + slot_rank
    outbound = (
        jnp.zeros((expert_total * capacity, model_width), jnp.bfloat16)
        .at[target]
        .set(jnp.repeat(normed, 2, axis=0))
    )
    outbound = outbound.reshape(expert_total, capacity, model_width)
    widened = lax.all_gather(
        lax.all_to_all(outbound, "sp", split_axis=0, concat_axis=0, tiled=True),
        "tp",
        axis=0,
        tiled=True,
    )
    flat_rows = widened.reshape(-1, widened.shape[-1])
    gate_out = jnp.dot(flat_rows, gate_weight, preferred_element_type=jnp.float32)
    up_out = jnp.dot(flat_rows, up_weight, preferred_element_type=jnp.float32)
    hidden = (jax.nn.silu(gate_out) * up_out).astype(jnp.bfloat16)
    partial_value = jnp.dot(
        hidden, down_weight, preferred_element_type=jnp.float32
    ).astype(jnp.bfloat16)
    partial_value = lax.optimization_barrier(
        partial_value.reshape(widened.shape[0], widened.shape[1], partial_value.shape[-1])
    ).astype(jnp.float32)
    summed = lax.psum_scatter(
        partial_value.astype(jnp.bfloat16), "tp", scatter_dimension=0, tiled=True
    )
    returned = lax.all_to_all(summed, "sp", split_axis=0, concat_axis=0, tiled=True)
    picked = jnp.take(returned.reshape(expert_total * capacity, model_width), target, axis=0)
    picked = picked.reshape(rows_here, 2, model_width).astype(jnp.float32)
    weighted = (
        expert_output_weight[:, 0:1] * picked[:, 0] + expert_output_weight[:, 1:2] * picked[:, 1]
    )
    return (wide_stream + weighted).astype(jnp.bfloat16)


def arrival_order(place, length):
    order = []
    for hops in range(1, length):
        if place - hops >= 0:
            order.append((hops, True))
        if place + hops < length:
            order.append((hops, False))
    return order


def select_by_place(place, choices):
    distinct = []
    for array in choices:
        if not any(array is d for d in distinct):
            distinct.append(array)
    out = distinct[0]
    for array in distinct[1:]:
        here = jnp.zeros((), jnp.bool_)
        for i, c in enumerate(choices):
            if c is array:
                here = here | (place == i)
        out = jnp.where(here, array, out)
    return out


def line_blocks(block, axis):
    length = lax.axis_size(axis)
    place = lax.axis_index(axis)
    from_left, from_right = [block], [block]
    for hops in range(1, length):
        rightward = [(i, i + 1) for i in range(hops - 1, length - 1)]
        leftward = [(length - 1 - i, length - 2 - i) for i in range(hops - 1, length - 1)]
        from_left.append(lax.ppermute(from_left[-1], axis, rightward))
        from_right.append(lax.ppermute(from_right[-1], axis, leftward))
    orders = [arrival_order(i, length) for i in range(length)]
    arrived = [block]
    for turn in range(length - 1):
        arrived.append(
            select_by_place(
                place,
                [
                    (from_left if orders[i][turn][1] else from_right)[orders[i][turn][0]]
                    for i in range(length)
                ],
            )
        )
    return arrived


def source_table(length):
    table = []
    for i in range(length):
        table.append(
            [i] + [i - hops if left else i + hops for hops, left in arrival_order(i, length)]
        )
    return table


def line_reduce(parts, axis):
    length = lax.axis_size(axis)
    place = lax.axis_index(axis)
    turn_of = [{d: t for t, d in enumerate(row)} for row in source_table(length)]

    def added(block, received):
        if received is None:
            return block
        return (block.astype(jnp.float32) + received.astype(jnp.float32)).astype(block.dtype)

    right, left = None, None
    for step in range(1, length):
        goes_right = [parts[turn_of[i][min(length - step + i, length - 1)]] for i in range(length)]
        goes_left = [parts[turn_of[i][max(step - length + i, 0)]] for i in range(length)]
        for i in range(step, length):
            goes_right[i] = goes_right[step - 1]
        for i in range(length - step):
            goes_left[i] = goes_left[length - step]
        right = lax.ppermute(
            added(select_by_place(place, goes_right), right),
            axis,
            [(i, i + 1) for i in range(min(step, length - 1))],
        )
        left = lax.ppermute(
            added(select_by_place(place, goes_left), left),
            axis,
            [(length - 1 - i, length - 2 - i) for i in range(min(step, length - 1))],
        )
    return parts[0].astype(jnp.float32) + right.astype(jnp.float32) + left.astype(jnp.float32)


def swapped(array, bit):
    return lax.ppermute(array, "sp", [(i, i ^ bit) for i in range(lax.axis_size("sp"))])


def dense_experts(
    wide_stream, normed, gate_weight, up_weight, down_weight, token_expert_choice, expert_output_weight
):
    rows_here, model_width = normed.shape
    expert_total = lax.axis_size("sp")
    length = lax.axis_size("tp")
    place = lax.axis_index("tp")
    mine = lax.axis_index("sp")
    capacity = 2 * rows_here // expert_total + 1
    slots = -(-4 * capacity // 8) * 8
    facts = jnp.concatenate(
        [token_expert_choice.astype(jnp.float32), expert_output_weight], axis=1
    ).T
    facts = lax.all_gather(lax.all_gather(facts, "tp"), "sp")
    blocks = line_blocks(normed, "tp")
    across = [swapped(b, 2) for b in blocks]
    sources = jnp.asarray(source_table(length), jnp.int32)[place]
    sums = []
    for turn in range(length):
        pair = [blocks[turn], across[turn]]
        four = [pair[0], swapped(pair[0], 1), pair[1], swapped(pair[1], 1)]
        rows = jnp.concatenate(four, axis=0)
        known = jnp.stack(
            [facts[mine ^ bit, sources[turn]] for bit in (0, 1, 2, 3)], axis=1
        ).reshape(4, 4 * rows_here)
        named = known[:2] == mine.astype(jnp.float32)
        weight = jnp.sum(jnp.where(named, known[2:], 0.0), axis=0)
        here = jnp.any(named, axis=0)
        rank = jnp.cumsum(here.astype(jnp.int32)) - 1
        slot = jnp.where(here, rank, -1)
        chosen = (jnp.arange(slots, dtype=jnp.int32)[:, None] == slot[None, :]).astype(jnp.bfloat16)
        taken = jnp.dot(chosen, rows, preferred_element_type=jnp.float32).astype(jnp.bfloat16)
        gate_out = jnp.dot(taken, gate_weight, preferred_element_type=jnp.float32)
        up_out = jnp.dot(taken, up_weight, preferred_element_type=jnp.float32)
        hidden = (jax.nn.silu(gate_out) * up_out).astype(jnp.bfloat16)
        result = jnp.dot(hidden, down_weight, preferred_element_type=jnp.float32).astype(
            jnp.bfloat16
        )
        spread = lax.dot_general(
            chosen, result, (((0,), (0,)), ((), ())), preferred_element_type=jnp.float32
        )
        sums.append((spread * weight[:, None]).astype(jnp.bfloat16).reshape(4, rows_here, model_width))

    def added(one, two):
        return (one.astype(jnp.float32) + two.astype(jnp.float32)).astype(jnp.bfloat16)

    parts = [None] * length
    for turn in reversed(range(length)):
        near = added(sums[turn][0], swapped(sums[turn][1], 1))
        far = added(sums[turn][2], swapped(sums[turn][3], 1))
        parts[turn] = added(near, swapped(far, 2))
    return (wide_stream + line_reduce(parts, "tp")).astype(jnp.bfloat16)


def local(
    residual,
    grouped_value_heads,
    output_gate_heads,
    projected_key_query,
    raw_step_size,
    step_size_bias,
    head_decay_logarithm,
    position_extra_decay,
    head_skip_weight,
    value_kernel_taps,
    key_query_kernel,
    head_norm_gain,
    output_matrix,
    expert_norm_gain,
    expert_gate_weight,
    expert_up_weight,
    expert_down_weight,
    token_expert_choice,
    expert_output_weight,
):
    lane_width = grouped_value_heads.shape[2]
    mixed_heads = mixed_rows(
        grouped_value_heads,
        output_gate_heads,
        projected_key_query,
        raw_step_size,
        step_size_bias,
        head_decay_logarithm,
        position_extra_decay,
        head_skip_weight,
        value_kernel_taps,
        key_query_kernel,
        head_norm_gain,
    )
    rows_here = residual.shape[0]
    model_width = output_matrix.shape[2]
    mix_out = lax.psum_scatter(
        jnp.dot(
            mixed_heads,
            output_matrix.reshape(2 * lane_width, model_width),
            preferred_element_type=jnp.float32,
        ).astype(jnp.bfloat16),
        "tp",
        scatter_dimension=0,
        tiled=True,
    ).astype(jnp.float32)
    stream = (residual.astype(jnp.float32) + mix_out).astype(jnp.bfloat16)
    wide_stream = stream.astype(jnp.float32)
    normed = (
        wide_stream
        * lax.rsqrt(jnp.mean(wide_stream * wide_stream, axis=1, keepdims=True) + EPSILON)
        * expert_norm_gain[None]
    ).astype(jnp.bfloat16)
    operands = (
        wide_stream,
        normed,
        expert_gate_weight[0],
        expert_up_weight[0],
        expert_down_weight[0],
        token_expert_choice,
        expert_output_weight,
    )
    if lax.axis_size("sp") == 4:
        return dense_experts(*operands)
    return routed_experts(*operands)


def solution(mesh):
    placed = (
        P(("grp", "sp", "tp"), None),
        P(("grp", "sp"), None, "tp"),
        P(("grp", "sp"), None, "tp"),
        P(("grp", "sp"), None),
        P(("grp", "sp"), None, "tp"),
        P(None, "tp"),
        P(None, "tp"),
        P(("grp", "sp")),
        P(None, "tp"),
        P(None, None, "tp"),
        P(),
        P(None, "tp"),
        P(None, "tp", None),
        P(),
        P("sp", None, "tp"),
        P("sp", None, "tp"),
        P("sp", "tp", None),
        P(("grp", "sp", "tp"), None),
        P(("grp", "sp", "tp"), None),
    )
    return jax.shard_map(
        local, mesh=mesh, in_specs=placed, out_specs=P(("grp", "sp", "tp"), None), check_vma=False
    )
```

```python
import functools

import jax
import jax.numpy as jnp
from jax import lax
from jax.experimental import pallas as pl
from jax.experimental.pallas import tpu as pltpu
from jax.sharding import PartitionSpec as P


HEAD_DIM = 64
STATE_ONE = 64
STATE_TWO = 128
BLOCK = 128


EPSILON = 1e-06


def passed_along(shard, axis, by):
    length = lax.axis_size(axis)
    pairs = [(i, i + by) for i in range(length) if 0 <= i + by < length]
    return lax.ppermute(shard, axis, pairs)


def high_rows(heads):
    return -(-2 * heads // 8) * 8


def widened(column, heads, width):
    rows = column.shape[0]
    return jnp.concatenate(
        [jnp.broadcast_to(column[:, h : h + 1], (rows, width)) for h in range(heads)], axis=1
    )


def spread_down(tall, first, heads, width):
    return jnp.concatenate(
        [jnp.broadcast_to(tall[first + h : first + h + 1], (1, width)) for h in range(heads)], axis=1
    )


def both_groups(tall, heads, width):
    return jnp.concatenate(
        [spread_down(tall, g * heads, heads, width) for g in range(2)], axis=1
    )


def states_kernel(
    heads,
    sizes,
    values_ref,
    keys_ref,
    rim_ref,
    value_taps_ref,
    key_taps_ref,
    steps_ref,
    facts_ref,
    extra_ref,
    x_ref,
    rows_ref,
    across_ref,
    down_ref,
    enter_one_ref,
    enter_two_ref,
    earlier_ref,
    packed_ref,
    tail_ref,
    one_ref,
    two_ref,
    sum_ref,
):
    step = pl.program_id(0)
    lanes = heads * HEAD_DIM
    taps = value_taps_ref.shape[0]

    @pl.when(step == 0)
    def _():
        tail_ref[...] = rim_ref[...].astype(jnp.float32)
        one_ref[...] = jnp.zeros_like(one_ref)
        two_ref[...] = jnp.zeros_like(two_ref)
        sum_ref[...] = jnp.zeros_like(sum_ref)

    here = jnp.concatenate(
        [values_ref[...].astype(jnp.float32), keys_ref[...].astype(jnp.float32)], axis=1
    )
    extended = jnp.concatenate([tail_ref[...], here], axis=0)
    tail_ref[...] = here[BLOCK - 8 :]
    weights = jnp.concatenate(
        [value_taps_ref[...].astype(jnp.float32), key_taps_ref[...].astype(jnp.float32)], axis=1
    )
    summed = jnp.zeros_like(here)
    for j in range(taps):
        first = 8 - (taps - 1) + j
        summed = summed + extended[first : first + BLOCK] * weights[j : j + 1]
    active = (summed * jax.nn.sigmoid(summed)).astype(jnp.bfloat16)
    x = active[:, : 2 * lanes]
    rows = active[:, 2 * lanes :]
    x_ref[...] = x
    rows_ref[...] = rows

    raw = steps_ref[...] + facts_ref[:, 0:1]
    stride = jnp.maximum(raw, 0.0) + jnp.log1p(jnp.exp(-jnp.abs(raw)))
    log_decay = extra_ref[...] - jnp.exp(facts_ref[:, 1:2]) * stride
    upto = (
        lax.broadcasted_iota(jnp.int32, (BLOCK, BLOCK), 0)
        <= lax.broadcasted_iota(jnp.int32, (BLOCK, BLOCK), 1)
    ).astype(jnp.float32)
    running = jnp.dot(
        log_decay, upto, preferred_element_type=jnp.float32, precision=lax.Precision.HIGHEST
    )
    end = running[:, BLOCK - 1 :]
    fading = jnp.exp(end - running) * stride
    high = running.shape[0]
    stacked = jnp.concatenate(
        [running, fading, jnp.exp(running)]
        + [jnp.zeros((BLOCK - 3 * high, BLOCK), jnp.float32)],
        axis=0,
    )
    down = stacked.T
    across_ref[...] = jnp.concatenate([running, stride], axis=0)
    down_ref[...] = down
    earlier_ref[...] = jnp.broadcast_to(
        jnp.exp(both_groups(sum_ref[...], heads, HEAD_DIM)), earlier_ref.shape
    )
    faded_end = jnp.exp(both_groups(end, heads, HEAD_DIM))
    bound = 0
    for g, (enter_ref, state_ref) in enumerate(((enter_one_ref, one_ref), (enter_two_ref, two_ref))):
        keys = rows[:, bound : bound + sizes[g]]
        bound += 2 * sizes[g]
        fade = widened(down[:, high + g * heads : high + (g + 1) * heads], heads, HEAD_DIM)
        scaled = (x[:, g * lanes : (g + 1) * lanes].astype(jnp.float32) * fade).astype(jnp.bfloat16)
        own = lax.dot_general(
            keys, scaled, (((0,), (0,)), ((), ())), preferred_element_type=jnp.float32
        )
        state = state_ref[...]
        enter_ref[0] = state
        state_ref[...] = state * faded_end[:, g * lanes : (g + 1) * lanes] + own
    total = sum_ref[...] + end
    sum_ref[...] = total

    @pl.when(step == pl.num_programs(0) - 1)
    def _():
        whole = both_groups(total, heads, HEAD_DIM)
        high_part = whole.astype(jnp.bfloat16)
        low_part = (whole - high_part.astype(jnp.float32)).astype(jnp.bfloat16)
        packed_ref[0 : sizes[0]] = one_ref[...].astype(jnp.bfloat16)
        packed_ref[sizes[0] : sizes[0] + sizes[1]] = two_ref[...].astype(jnp.bfloat16)
        packed_ref[sizes[0] + sizes[1] :] = jnp.concatenate(
            [
                jnp.broadcast_to(part[:, g * lanes : (g + 1) * lanes].astype(jnp.float32), (4, lanes))
                for g in range(2)
                for part in (high_part, low_part)
            ],
            axis=0,
        ).astype(jnp.bfloat16)


def near_kernel(heads, sizes, x_ref, rows_ref, across_ref, down_ref, facts_ref, near_ref):
    high = across_ref.shape[0] // 2
    later = lax.broadcasted_iota(jnp.int32, (BLOCK, BLOCK), 0) >= lax.broadcasted_iota(
        jnp.int32, (BLOCK, BLOCK), 1
    )
    skip = both_groups(facts_ref[:, 2:3], heads, HEAD_DIM)
    bound = 0
    out = []
    for g in range(2):
        keys = rows_ref[:, bound : bound + sizes[g]]
        queries = rows_ref[:, bound + sizes[g] : bound + 2 * sizes[g]]
        bound += 2 * sizes[g]
        scores = lax.dot_general(
            queries, keys, (((1,), (1,)), ((), ())), preferred_element_type=jnp.float32
        )
        for h in range(heads):
            i = g * heads + h
            spread = jnp.where(later, down_ref[:, i : i + 1] - across_ref[i : i + 1], -1e30)
            weights = scores * jnp.exp(spread) * across_ref[high + i : high + i + 1]
            x = x_ref[:, i * HEAD_DIM : (i + 1) * HEAD_DIM]
            out.append(
                jnp.dot(weights.astype(jnp.bfloat16), x, preferred_element_type=jnp.float32)
            )
    near_ref[...] = jnp.concatenate(out, axis=1) + skip * x_ref[...].astype(jnp.float32)


def mixed_values(heads, sizes, prior_count, refs):
    priors = refs[:prior_count]
    (
        near_ref,
        rows_ref,
        down_ref,
        enter_one_ref,
        enter_two_ref,
        earlier_ref,
        gate_ref,
        gain_ref,
        one_ref,
        two_ref,
    ) = refs[prior_count:]
    lanes = heads * HEAD_DIM
    high = high_rows(heads)

    @pl.when(pl.program_id(0) == 0)
    def _():
        base = sizes[0] + sizes[1]
        for g, state_ref in enumerate((one_ref, two_ref)):
            state = jnp.zeros_like(state_ref)
            first = g * sizes[0]
            for prior in reversed(priors):
                facts = prior[base:].astype(jnp.float32)
                decay = facts[8 * g : 8 * g + 1] + facts[8 * g + 4 : 8 * g + 5]
                own = prior[first : first + sizes[g]].astype(jnp.float32)
                state = state * jnp.exp(decay) + own
            state_ref[...] = state

    bound = 0
    out = []
    for g, (enter_ref, state_ref) in enumerate(((enter_one_ref, one_ref), (enter_two_ref, two_ref))):
        queries = rows_ref[:, bound + sizes[g] : bound + 2 * sizes[g]]
        bound += 2 * sizes[g]
        here = slice(g * lanes, (g + 1) * lanes)
        entering = enter_ref[0] + state_ref[...] * earlier_ref[0:1, here]
        far = jnp.dot(
            queries, entering.astype(jnp.bfloat16), preferred_element_type=jnp.float32
        )
        reach = down_ref[:, 2 * high + g * heads : 2 * high + (g + 1) * heads]
        gate = gate_ref[:, here].astype(jnp.float32)
        total = near_ref[:, here] + far * widened(reach, heads, HEAD_DIM)
        gated = total * (gate * jax.nn.sigmoid(gate))
        squares = gated * gated
        means = jnp.concatenate(
            [
                jnp.sum(squares[:, h * HEAD_DIM : (h + 1) * HEAD_DIM], axis=1, keepdims=True)
                for h in range(heads)
            ],
            axis=1,
        ) * (1.0 / HEAD_DIM)
        scale = widened(lax.rsqrt(means + EPSILON), heads, HEAD_DIM)
        out.append((gated * scale * gain_ref[:, here]).astype(jnp.bfloat16))
    return jnp.concatenate(out, axis=1)


def mixed_kernel(heads, sizes, prior_count, *refs):
    inputs = prior_count + 8
    refs[inputs][...] = mixed_values(heads, sizes, prior_count, refs[:inputs] + refs[inputs + 1 :])


def projected_kernel(heads, sizes, prior_count, turns, order_ref, *refs):
    inputs = prior_count + 8
    matrix_ref, outs = refs[inputs], refs[inputs + 1 : inputs + 1 + turns]
    mixed = mixed_values(heads, sizes, prior_count, refs[:inputs] + refs[inputs + 1 + turns :])
    product = jnp.dot(mixed, matrix_ref[...], preferred_element_type=jnp.float32)
    for turn, out_ref in enumerate(outs):

        @pl.when(pl.program_id(0) == turn)
        def _(out_ref=out_ref):
            out_ref[...] = product.astype(jnp.bfloat16)


def mixed_rows(
    grouped_value_heads,
    output_gate_heads,
    projected_key_query,
    raw_step_size,
    step_size_bias,
    head_decay_logarithm,
    position_extra_decay,
    head_skip_weight,
    value_kernel_taps,
    key_query_kernel,
    head_norm_gain,
    output_matrix,
    order,
):
    positions, _, lanes = grouped_value_heads.shape
    heads = lanes // HEAD_DIM
    high = high_rows(heads)
    sizes = (STATE_ONE, STATE_TWO)
    width = key_query_kernel.shape[1]
    blocks = positions // BLOCK
    last = grouped_value_heads[positions - 8 :].reshape(8, 2 * lanes)
    rim = passed_along(
        jnp.concatenate([last, projected_key_query[positions - 8 :]], axis=1), "sp", 1
    )
    values = grouped_value_heads.reshape(positions, 2 * lanes)
    facts = jnp.stack(
        [step_size_bias.reshape(-1), head_decay_logarithm.reshape(-1), head_skip_weight.reshape(-1)],
        axis=1,
    )
    facts = jnp.pad(facts, ((0, high - 2 * heads), (0, 0)))
    steps = raw_step_size.reshape(positions, 2 * heads).T.astype(jnp.float32)
    steps = jnp.pad(steps, ((0, high - 2 * heads), (0, 0)))

    def by_block(rows, columns):
        return pl.BlockSpec((rows, columns), lambda k: (k, 0))

    def along(rows):
        return pl.BlockSpec((rows, BLOCK), lambda k: (0, k))

    def fixed(*shape):
        return pl.BlockSpec(shape, lambda k: (0,) * len(shape))

    def per_block(*shape):
        return pl.BlockSpec((1, *shape), lambda k: (k,) + (0,) * len(shape))

    f32, bf16 = jnp.float32, jnp.bfloat16
    packed_rows = sizes[0] + sizes[1] + 16
    x, rows, across, down, enter_one, enter_two, earlier, packed = pl.pallas_call(
        functools.partial(states_kernel, heads, sizes),
        grid=(blocks,),
        in_specs=[
            by_block(BLOCK, 2 * lanes),
            by_block(BLOCK, width),
            fixed(8, 2 * lanes + width),
            fixed(value_kernel_taps.shape[0], 2 * lanes),
            fixed(*key_query_kernel.shape),
            along(high),
            fixed(high, 3),
            along(1),
        ],
        out_specs=[
            by_block(BLOCK, 2 * lanes),
            by_block(BLOCK, width),
            along(2 * high),
            by_block(BLOCK, BLOCK),
            per_block(sizes[0], lanes),
            per_block(sizes[1], lanes),
            by_block(8, 2 * lanes),
            fixed(packed_rows, lanes),
        ],
        out_shape=[
            jax.ShapeDtypeStruct((positions, 2 * lanes), bf16),
            jax.ShapeDtypeStruct((positions, width), bf16),
            jax.ShapeDtypeStruct((2 * high, positions), f32),
            jax.ShapeDtypeStruct((positions, BLOCK), f32),
            jax.ShapeDtypeStruct((blocks, sizes[0], lanes), f32),
            jax.ShapeDtypeStruct((blocks, sizes[1], lanes), f32),
            jax.ShapeDtypeStruct((8 * blocks, 2 * lanes), f32),
            jax.ShapeDtypeStruct((packed_rows, lanes), bf16),
        ],
        scratch_shapes=[
            pltpu.VMEM((8, 2 * lanes + width), f32),
            pltpu.VMEM((sizes[0], lanes), f32),
            pltpu.VMEM((sizes[1], lanes), f32),
            pltpu.VMEM((high, 1), f32),
        ],
        name="states",
    )(
        values,
        projected_key_query,
        rim,
        value_kernel_taps.reshape(-1, 2 * lanes),
        key_query_kernel,
        steps,
        facts,
        position_extra_decay[None],
    )
    priors = [passed_along(packed, "sp", by) for by in range(1, lax.axis_size("sp"))]
    near = pl.pallas_call(
        functools.partial(near_kernel, heads, sizes),
        grid=(blocks,),
        in_specs=[
            by_block(BLOCK, 2 * lanes),
            by_block(BLOCK, width),
            along(2 * high),
            by_block(BLOCK, BLOCK),
            fixed(high, 3),
        ],
        out_specs=by_block(BLOCK, 2 * lanes),
        out_shape=jax.ShapeDtypeStruct((positions, 2 * lanes), f32),
        name="near",
    )(x, rows, across, down, facts)
    operands = (
        *priors,
        near,
        rows,
        down,
        enter_one,
        enter_two,
        earlier,
        output_gate_heads.reshape(positions, 2 * lanes),
        head_norm_gain.reshape(1, 2 * lanes),
    )
    scratch_shapes = [pltpu.VMEM((sizes[0], lanes), f32), pltpu.VMEM((sizes[1], lanes), f32)]
    if order is None:
        return pl.pallas_call(
            functools.partial(mixed_kernel, heads, sizes, len(priors)),
            grid=(blocks,),
            in_specs=[fixed(packed_rows, lanes) for _ in priors]
            + [
                by_block(BLOCK, 2 * lanes),
                by_block(BLOCK, width),
                by_block(BLOCK, BLOCK),
                per_block(sizes[0], lanes),
                per_block(sizes[1], lanes),
                by_block(8, 2 * lanes),
                by_block(BLOCK, 2 * lanes),
                fixed(1, 2 * lanes),
            ],
            out_specs=by_block(BLOCK, 2 * lanes),
            out_shape=jax.ShapeDtypeStruct((positions, 2 * lanes), bf16),
            scratch_shapes=scratch_shapes,
            name="mixed",
        )(*operands)

    def whole(*shape):
        return pl.BlockSpec(shape, lambda k, order: (0,) * len(shape))

    def chosen(rows, columns):
        return pl.BlockSpec((rows, columns), lambda k, order: (order[k], 0))

    def chosen_state(*shape):
        return pl.BlockSpec((1, *shape), lambda k, order: (order[k],) + (0,) * len(shape))

    model_width = output_matrix.shape[2]
    return pl.pallas_call(
        functools.partial(projected_kernel, heads, sizes, len(priors), blocks),
        grid_spec=pltpu.PrefetchScalarGridSpec(
            num_scalar_prefetch=1,
            grid=(blocks,),
            in_specs=[whole(packed_rows, lanes) for _ in priors]
            + [
                chosen(BLOCK, 2 * lanes),
                chosen(BLOCK, width),
                chosen(BLOCK, BLOCK),
                chosen_state(sizes[0], lanes),
                chosen_state(sizes[1], lanes),
                chosen(8, 2 * lanes),
                chosen(BLOCK, 2 * lanes),
                whole(1, 2 * lanes),
                whole(2 * lanes, model_width),
            ],
            out_specs=[whole(BLOCK, model_width)] * blocks,
            scratch_shapes=scratch_shapes,
        ),
        out_shape=[jax.ShapeDtypeStruct((BLOCK, model_width), bf16)] * blocks,
        name="projected",
    )(order, *operands, output_matrix.reshape(2 * lanes, model_width))


def routed_experts(
    wide_stream, normed, gate_weight, up_weight, down_weight, token_expert_choice, expert_output_weight
):
    rows_here, model_width = normed.shape
    expert_total = lax.axis_size("sp")
    capacity = 2 * rows_here // expert_total + 1
    flat_ids = token_expert_choice.reshape(-1)
    matches = (flat_ids[:, None] == jnp.arange(expert_total, dtype=jnp.int32)[None, :]).astype(
        jnp.int32
    )
    slot_rank = jnp.sum((jnp.cumsum(matches, axis=0) - matches) * matches, axis=1)
    target = flat_ids * capacity + slot_rank
    outbound = (
        jnp.zeros((expert_total * capacity, model_width), jnp.bfloat16)
        .at[target]
        .set(jnp.repeat(normed, 2, axis=0))
    )
    outbound = outbound.reshape(expert_total, capacity, model_width)
    widened = lax.all_gather(
        lax.all_to_all(outbound, "sp", split_axis=0, concat_axis=0, tiled=True),
        "tp",
        axis=0,
        tiled=True,
    )
    flat_rows = widened.reshape(-1, widened.shape[-1])
    gate_out = jnp.dot(flat_rows, gate_weight, preferred_element_type=jnp.float32)
    up_out = jnp.dot(flat_rows, up_weight, preferred_element_type=jnp.float32)
    hidden = (jax.nn.silu(gate_out) * up_out).astype(jnp.bfloat16)
    partial_value = jnp.dot(
        hidden, down_weight, preferred_element_type=jnp.float32
    ).astype(jnp.bfloat16)
    partial_value = lax.optimization_barrier(
        partial_value.reshape(widened.shape[0], widened.shape[1], partial_value.shape[-1])
    ).astype(jnp.float32)
    summed = lax.psum_scatter(
        partial_value.astype(jnp.bfloat16), "tp", scatter_dimension=0, tiled=True
    )
    returned = lax.all_to_all(summed, "sp", split_axis=0, concat_axis=0, tiled=True)
    picked = jnp.take(returned.reshape(expert_total * capacity, model_width), target, axis=0)
    picked = picked.reshape(rows_here, 2, model_width).astype(jnp.float32)
    weighted = (
        expert_output_weight[:, 0:1] * picked[:, 0] + expert_output_weight[:, 1:2] * picked[:, 1]
    )
    return (wide_stream + weighted).astype(jnp.bfloat16)


def swapped(array, bit):
    return lax.ppermute(array, "sp", [(i, i ^ bit) for i in range(lax.axis_size("sp"))])


def expert_kernel(region, own_ref, *refs):
    blocks = refs[:4]
    keep_ref, send_ref = refs[7:9]
    gate_ref, up_ref, back_ref, arrived = refs[9:]
    fetches = [
        pltpu.make_async_copy(source, target, arrived.at[i])
        for i, (source, target) in enumerate(zip(refs[4:7], (gate_ref, up_ref, back_ref)))
    ]
    for fetch in fetches:
        fetch.start()
    width = gate_ref.shape[0]
    rows = blocks[0].shape[0]
    own = own_ref[0].astype(jnp.float32)
    place = lax.broadcasted_iota(jnp.int32, (region, rows), 0).astype(jnp.float32)
    before = (
        lax.broadcasted_iota(jnp.int32, (rows, rows), 0)
        < lax.broadcasted_iota(jnp.int32, (rows, rows), 1)
    ).astype(jnp.float32)
    named, weights = [], []
    for block in blocks:
        facts = block[:, width:].astype(jnp.float32).T
        hits = (facts[0:2] == own).astype(jnp.float32)
        named.append(hits[0:1] + hits[1:2])
        weights.append(
            hits[0:1] * (facts[2:3] + facts[4:5]) + hits[1:2] * (facts[3:4] + facts[5:6])
        )
    named = jnp.concatenate(named + [jnp.zeros((4, rows), jnp.float32)], axis=0)
    inner = jnp.dot(named, before, preferred_element_type=jnp.float32)
    slot = jnp.where(named > 0, inner, -1.0)
    taken = []
    for i, block in enumerate(blocks):
        chosen = (place == slot[i : i + 1]).astype(jnp.bfloat16)
        taken.append(jnp.dot(chosen, block[:, :width], preferred_element_type=jnp.float32))
    taken = jnp.concatenate(taken, axis=0).astype(jnp.bfloat16)
    down = jnp.concatenate(
        [slot[0:4]] + weights + [jnp.zeros((rows - 8, rows), jnp.float32)], axis=0
    ).T
    fetches[0].wait()
    gate = jnp.dot(taken, gate_ref[...], preferred_element_type=jnp.float32)
    fetches[1].wait()
    up = jnp.dot(taken, up_ref[...], preferred_element_type=jnp.float32)
    hidden = (gate * jax.nn.sigmoid(gate) * up).astype(jnp.bfloat16)
    fetches[2].wait()
    result = jnp.dot(hidden, back_ref[...], preferred_element_type=jnp.float32)
    place = lax.broadcasted_iota(jnp.int32, (rows, region), 1).astype(jnp.float32)
    for i in range(4):
        chosen = (place == down[:, i : i + 1]).astype(jnp.bfloat16)
        spread = jnp.dot(
            chosen,
            result[i * region : (i + 1) * region].astype(jnp.bfloat16),
            preferred_element_type=jnp.float32,
        )
        out_ref = (keep_ref, send_ref)[i // 2]
        out_ref[i % 2 * rows : (i % 2 + 1) * rows] = (spread * down[:, 4 + i : 5 + i]).astype(
            jnp.bfloat16
        )


def run_expert(blocks, own, gate_weight, up_weight, down_weight, capacity):
    rows = blocks[0].shape[0]
    width, hidden = gate_weight.shape
    region = -(-capacity // 8) * 8
    vmem = pl.BlockSpec(memory_space=pltpu.VMEM)
    return pl.pallas_call(
        functools.partial(expert_kernel, region),
        in_specs=[pl.BlockSpec(memory_space=pltpu.SMEM)] + [vmem] * 4 + [pl.BlockSpec(memory_space=pl.ANY)] * 3,
        out_specs=[vmem] * 2,
        out_shape=[jax.ShapeDtypeStruct((2 * rows, width), jnp.bfloat16)] * 2,
        scratch_shapes=[
            pltpu.VMEM((width, hidden), jnp.bfloat16),
            pltpu.VMEM((width, hidden), jnp.bfloat16),
            pltpu.VMEM((hidden, width), jnp.bfloat16),
            pltpu.SemaphoreType.DMA((3,)),
        ],
        cost_estimate=pl.CostEstimate(
            flops=24 * region * width * hidden,
            bytes_accessed=6 * width * hidden,
            transcendentals=4 * region * hidden,
        ),
        name="expert",
    )(own[None], *blocks, gate_weight, up_weight, down_weight)


def added(block, *received):
    total = block.astype(jnp.float32)
    for other in received:
        if other is not None:
            total = total + other.astype(jnp.float32)
    return total.astype(jnp.bfloat16)


def stream_kernel(
    residual_ref, own_ref, one_ref, two_ref, three_ref, gain_ref, facts_ref, stream_ref, rows_ref
):
    total = own_ref[...].astype(jnp.float32) + residual_ref[...].astype(jnp.float32)
    for ref in (one_ref, two_ref, three_ref):
        total = total + ref[...].astype(jnp.float32)
    stream = total.astype(jnp.bfloat16)
    stream_ref[...] = stream
    wide = stream.astype(jnp.float32)
    scale = lax.rsqrt(jnp.mean(wide * wide, axis=1, keepdims=True) + EPSILON)
    width = wide.shape[1]
    rows_ref[:, :width] = (wide * scale * gain_ref[...]).astype(jnp.bfloat16)
    rows_ref[:, width:] = facts_ref[...]


def stream_and_rows(residual, parts, gain, token_expert_choice, expert_output_weight):
    rows, width = residual.shape
    high = expert_output_weight.astype(jnp.bfloat16)
    low = (expert_output_weight - high.astype(jnp.float32)).astype(jnp.bfloat16)
    facts = jnp.concatenate([token_expert_choice.astype(jnp.bfloat16), high, low], axis=1)
    facts = jnp.pad(facts, ((0, 0), (0, rows - facts.shape[1])))
    return pl.pallas_call(
        stream_kernel,
        out_shape=[
            jax.ShapeDtypeStruct((rows, width), jnp.bfloat16),
            jax.ShapeDtypeStruct((rows, width + rows), jnp.bfloat16),
        ],
        name="stream",
    )(residual, *parts, gain[None], facts)


SWAPS = [(0, 1), (1, 0), (2, 3), (3, 2)]
MIDDLE = [(1, 2), (2, 1)]
ENDS = [(0, 3), (3, 0)]
OUTWARD = [(1, 0), (2, 3)]
INWARD = [(0, 1), (3, 2)]
ARRIVALS = [[0, 1, 3, 2], [1, 0, 2, 3], [2, 3, 1, 0], [3, 2, 0, 1]]


def line_sum(parts):
    ends = lax.ppermute(parts[2], "tp", ENDS)
    middle = lax.ppermute(parts[3], "tp", MIDDLE)
    inward = lax.ppermute(parts[3], "tp", INWARD)
    pair = lax.ppermute(added(parts[1], middle), "tp", SWAPS)
    middle_two = lax.ppermute(added(parts[2], inward), "tp", MIDDLE)
    return parts[0], ends, pair, middle_two


def final_kernel(stream_ref, *refs):
    out_ref = refs[-1]
    total = stream_ref[...].astype(jnp.float32)
    for ref in refs[:-1]:
        total = total + ref[...].astype(jnp.float32)
    out_ref[...] = total.astype(jnp.bfloat16)


def near_kernel_sum(keep_ref, back_ref, out_ref):
    total = keep_ref[...].astype(jnp.float32) + back_ref[...].astype(jnp.float32)
    out_ref[...] = total.astype(jnp.bfloat16)


def near_added(keep, back):
    rows, width = keep.shape
    half = pl.BlockSpec((rows // 2, width), lambda k: (0, 0))
    return pl.pallas_call(
        near_kernel_sum,
        grid=(1,),
        in_specs=[half, half],
        out_specs=half,
        out_shape=jax.ShapeDtypeStruct((rows // 2, width), jnp.bfloat16),
        name="near_sum",
    )(keep, back)


def dense_experts(stream, normed, gate_weight, up_weight, down_weight):
    rows = normed.shape[0]
    capacity = 2 * rows // lax.axis_size("sp") + 1
    place = lax.axis_index("tp")
    mine = lax.axis_index("sp").astype(jnp.int32)
    inner = (place == 1) | (place == 2)

    far = [swapped(normed, 2)]
    from_pair = lax.ppermute(normed, "tp", SWAPS)
    second = lax.ppermute(normed, "tp", MIDDLE + ENDS)
    middle_two = lax.ppermute(from_pair, "tp", MIDDLE)
    outer_two = lax.ppermute(second, "tp", OUTWARD)
    third = jnp.where(inner, middle_two, outer_two)
    blocks = [normed, from_pair, second, third]
    sums = []
    near_other, far_other = [], []
    for turn in range(4):
        if turn:
            far.append(swapped(blocks[turn], 2))
        near_other.append(swapped(blocks[turn], 1))
        far_other.append(swapped(far[turn], 1))
    near_sums, far_sums = [], []
    for turn in range(4):
        keep, send = run_expert(
            [blocks[turn], far[turn], near_other[turn], far_other[turn]],
            mine,
            gate_weight,
            up_weight,
            down_weight,
            capacity,
        )
        back = swapped(send, 1)
        near_sums.append((keep[:rows], back[:rows]))
        if turn == 3:
            near_last = near_added(keep, back)
        far_sums.append(added(keep[rows:], back[rows:]))
    crossed = [swapped(far_sums[turn], 2) for turn in range(4)]
    parts = [None, added(*near_sums[1], crossed[1])]
    parts.append(lax.optimization_barrier(added(*near_sums[2], crossed[2])))
    parts.append(lax.optimization_barrier(added(near_last, crossed[3])))
    sums = line_sum(parts)[1:]
    return pl.pallas_call(
        final_kernel,
        out_shape=jax.ShapeDtypeStruct(stream.shape, jnp.bfloat16),
        name="final",
    )(stream, *near_sums[0], crossed[0], *sums)


def local(
    residual,
    grouped_value_heads,
    output_gate_heads,
    projected_key_query,
    raw_step_size,
    step_size_bias,
    head_decay_logarithm,
    position_extra_decay,
    head_skip_weight,
    value_kernel_taps,
    key_query_kernel,
    head_norm_gain,
    output_matrix,
    expert_norm_gain,
    expert_gate_weight,
    expert_up_weight,
    expert_down_weight,
    token_expert_choice,
    expert_output_weight,
):
    lane_width = grouped_value_heads.shape[2]
    dense = lax.axis_size("sp") == 4 and lax.axis_size("tp") == 4
    order = jnp.asarray(ARRIVALS, jnp.int32)[lax.axis_index("tp")] if dense else None
    mixed_heads = mixed_rows(
        grouped_value_heads,
        output_gate_heads,
        projected_key_query,
        raw_step_size,
        step_size_bias,
        head_decay_logarithm,
        position_extra_decay,
        head_skip_weight,
        value_kernel_taps,
        key_query_kernel,
        head_norm_gain,
        output_matrix,
        order,
    )
    weights = (expert_gate_weight[0], expert_up_weight[0], expert_down_weight[0])
    if dense:
        stream, normed = stream_and_rows(
            residual,
            line_sum(mixed_heads),
            expert_norm_gain,
            token_expert_choice,
            expert_output_weight,
        )
        return dense_experts(stream, normed, *weights)
    model_width = output_matrix.shape[2]
    mix_out = lax.psum_scatter(
        jnp.dot(
            mixed_heads,
            output_matrix.reshape(2 * lane_width, model_width),
            preferred_element_type=jnp.float32,
        ).astype(jnp.bfloat16),
        "tp",
        scatter_dimension=0,
        tiled=True,
    ).astype(jnp.float32)
    stream = (residual.astype(jnp.float32) + mix_out).astype(jnp.bfloat16)
    wide_stream = stream.astype(jnp.float32)
    normed = (
        wide_stream
        * lax.rsqrt(jnp.mean(wide_stream * wide_stream, axis=1, keepdims=True) + EPSILON)
        * expert_norm_gain[None]
    ).astype(jnp.bfloat16)
    return routed_experts(wide_stream, normed, *weights, token_expert_choice, expert_output_weight)


def solution(mesh):
    placed = (
        P(("grp", "sp", "tp"), None),
        P(("grp", "sp"), None, "tp"),
        P(("grp", "sp"), None, "tp"),
        P(("grp", "sp"), None),
        P(("grp", "sp"), None, "tp"),
        P(None, "tp"),
        P(None, "tp"),
        P(("grp", "sp")),
        P(None, "tp"),
        P(None, None, "tp"),
        P(),
        P(None, "tp"),
        P(None, "tp", None),
        P(),
        P("sp", None, "tp"),
        P("sp", None, "tp"),
        P("sp", "tp", None),
        P(("grp", "sp", "tp"), None),
        P(("grp", "sp", "tp"), None),
    )

    return jax.shard_map(
        local, mesh=mesh, in_specs=placed, out_specs=P(("grp", "sp", "tp"), None), check_vma=False
    )
```

```python
import functools

import jax
import jax.numpy as jnp
from jax import lax
from jax.experimental import pallas as pl
from jax.experimental.pallas import tpu as pltpu
from jax.sharding import PartitionSpec as P


HEAD_DIM = 64
STATE_ONE = 64
STATE_TWO = 128
BLOCK = 128


EPSILON = 1e-06


def passed_along(shard, axis, by):
    length = lax.axis_size(axis)
    pairs = [(i, i + by) for i in range(length) if 0 <= i + by < length]
    return lax.ppermute(shard, axis, pairs)


def high_rows(heads):
    return -(-2 * heads // 8) * 8


def widened(column, heads, width):
    rows = column.shape[0]
    return jnp.concatenate(
        [jnp.broadcast_to(column[:, h : h + 1], (rows, width)) for h in range(heads)], axis=1
    )


def spread_down(tall, first, heads, width):
    return jnp.concatenate(
        [jnp.broadcast_to(tall[first + h : first + h + 1], (1, width)) for h in range(heads)], axis=1
    )


def both_groups(tall, heads, width):
    return jnp.concatenate(
        [spread_down(tall, g * heads, heads, width) for g in range(2)], axis=1
    )


def head_facts(facts_ref, kind, high):
    heads = facts_ref.shape[1]
    both = jnp.concatenate(
        [facts_ref[2 * kind : 2 * kind + 1], facts_ref[2 * kind + 1 : 2 * kind + 2]], axis=1
    )
    if high > 2 * heads:
        both = jnp.concatenate([both, jnp.zeros((1, high - 2 * heads), jnp.float32)], axis=1)
    same = lax.broadcasted_iota(jnp.int32, (high, high), 0) == lax.broadcasted_iota(
        jnp.int32, (high, high), 1
    )
    return jnp.sum(jnp.where(same, jnp.broadcast_to(both, (high, high)), 0.0), axis=1, keepdims=True)


def states_kernel(
    heads,
    sizes,
    values_ref,
    keys_ref,
    rim_ref,
    value_taps_ref,
    key_taps_ref,
    steps_ref,
    facts_ref,
    extra_ref,
    x_ref,
    rows_ref,
    across_ref,
    down_ref,
    enter_one_ref,
    enter_two_ref,
    earlier_ref,
    packed_ref,
    tail_ref,
    one_ref,
    two_ref,
    sum_ref,
):
    step = pl.program_id(0)
    lanes = heads * HEAD_DIM
    taps = value_taps_ref.shape[0]

    @pl.when(step == 0)
    def _():
        tail_ref[...] = rim_ref[...].astype(jnp.float32)
        one_ref[...] = jnp.zeros_like(one_ref)
        two_ref[...] = jnp.zeros_like(two_ref)
        sum_ref[...] = jnp.zeros_like(sum_ref)

    here = jnp.concatenate(
        [values_ref[:, g].astype(jnp.float32) for g in range(2)]
        + [keys_ref[...].astype(jnp.float32)],
        axis=1,
    )
    extended = jnp.concatenate([tail_ref[...], here], axis=0)
    tail_ref[...] = here[BLOCK - 8 :]
    weights = jnp.concatenate(
        [value_taps_ref[:, g].astype(jnp.float32) for g in range(2)]
        + [key_taps_ref[...].astype(jnp.float32)],
        axis=1,
    )
    summed = jnp.zeros_like(here)
    for j in range(taps):
        first = 8 - (taps - 1) + j
        summed = summed + extended[first : first + BLOCK] * weights[j : j + 1]
    active = (summed * jax.nn.sigmoid(summed)).astype(jnp.bfloat16)
    x = active[:, : 2 * lanes]
    rows = active[:, 2 * lanes :]
    x_ref[...] = x
    rows_ref[...] = rows

    high = high_rows(heads)
    raw = [steps_ref[g].astype(jnp.float32) for g in range(2)]
    if high > 2 * heads:
        raw.append(jnp.zeros((high - 2 * heads, BLOCK), jnp.float32))
    raw = jnp.concatenate(raw, axis=0) + head_facts(facts_ref, 0, high)
    stride = jnp.maximum(raw, 0.0) + jnp.log1p(jnp.exp(-jnp.abs(raw)))
    log_decay = extra_ref[...] - jnp.exp(head_facts(facts_ref, 1, high)) * stride
    upto = (
        lax.broadcasted_iota(jnp.int32, (BLOCK, BLOCK), 0)
        <= lax.broadcasted_iota(jnp.int32, (BLOCK, BLOCK), 1)
    ).astype(jnp.float32)
    running = jnp.dot(
        log_decay, upto, preferred_element_type=jnp.float32, precision=lax.Precision.HIGHEST
    )
    end = running[:, BLOCK - 1 :]
    fading = jnp.exp(end - running) * stride
    stacked = jnp.concatenate(
        [running, fading, jnp.exp(running)]
        + [jnp.zeros((BLOCK - 3 * high, BLOCK), jnp.float32)],
        axis=0,
    )
    down = stacked.T
    across_ref[...] = jnp.concatenate([running, stride], axis=0)
    down_ref[...] = down
    earlier_ref[...] = jnp.broadcast_to(
        jnp.exp(both_groups(sum_ref[...], heads, HEAD_DIM)), earlier_ref.shape
    )
    faded_end = jnp.exp(both_groups(end, heads, HEAD_DIM))
    bound = 0
    for g, (enter_ref, state_ref) in enumerate(((enter_one_ref, one_ref), (enter_two_ref, two_ref))):
        keys = rows[:, bound : bound + sizes[g]]
        bound += 2 * sizes[g]
        fade = widened(down[:, high + g * heads : high + (g + 1) * heads], heads, HEAD_DIM)
        scaled = (x[:, g * lanes : (g + 1) * lanes].astype(jnp.float32) * fade).astype(jnp.bfloat16)
        own = lax.dot_general(
            keys, scaled, (((0,), (0,)), ((), ())), preferred_element_type=jnp.float32
        )
        state = state_ref[...]
        enter_ref[0] = state
        state_ref[...] = state * faded_end[:, g * lanes : (g + 1) * lanes] + own
    total = sum_ref[...] + end
    sum_ref[...] = total

    @pl.when(step == pl.num_programs(0) - 1)
    def _():
        whole = both_groups(total, heads, HEAD_DIM)
        high_part = whole.astype(jnp.bfloat16)
        low_part = (whole - high_part.astype(jnp.float32)).astype(jnp.bfloat16)
        packed_ref[0 : sizes[0]] = one_ref[...].astype(jnp.bfloat16)
        packed_ref[sizes[0] : sizes[0] + sizes[1]] = two_ref[...].astype(jnp.bfloat16)
        packed_ref[sizes[0] + sizes[1] :] = jnp.concatenate(
            [
                jnp.broadcast_to(part[:, g * lanes : (g + 1) * lanes].astype(jnp.float32), (4, lanes))
                for g in range(2)
                for part in (high_part, low_part)
            ],
            axis=0,
        ).astype(jnp.bfloat16)


def near_kernel(heads, sizes, x_ref, rows_ref, across_ref, down_ref, facts_ref, near_ref):
    high = across_ref.shape[0] // 2
    later = lax.broadcasted_iota(jnp.int32, (BLOCK, BLOCK), 0) >= lax.broadcasted_iota(
        jnp.int32, (BLOCK, BLOCK), 1
    )
    skip = both_groups(head_facts(facts_ref, 2, high), heads, HEAD_DIM)
    bound = 0
    out = []
    for g in range(2):
        keys = rows_ref[:, bound : bound + sizes[g]]
        queries = rows_ref[:, bound + sizes[g] : bound + 2 * sizes[g]]
        bound += 2 * sizes[g]
        scores = lax.dot_general(
            queries, keys, (((1,), (1,)), ((), ())), preferred_element_type=jnp.float32
        )
        for h in range(heads):
            i = g * heads + h
            spread = jnp.where(later, down_ref[:, i : i + 1] - across_ref[i : i + 1], -1e30)
            weights = scores * jnp.exp(spread) * across_ref[high + i : high + i + 1]
            x = x_ref[:, i * HEAD_DIM : (i + 1) * HEAD_DIM]
            out.append(
                jnp.dot(weights.astype(jnp.bfloat16), x, preferred_element_type=jnp.float32)
            )
    near_ref[...] = jnp.concatenate(out, axis=1) + skip * x_ref[...].astype(jnp.float32)


def mixed_values(heads, sizes, prior_count, refs):
    priors = refs[:prior_count]
    (
        near_ref,
        rows_ref,
        down_ref,
        enter_one_ref,
        enter_two_ref,
        earlier_ref,
        gate_ref,
        gain_ref,
        one_ref,
        two_ref,
    ) = refs[prior_count:]
    lanes = heads * HEAD_DIM
    high = high_rows(heads)

    @pl.when(pl.program_id(0) == 0)
    def _():
        base = sizes[0] + sizes[1]
        for g, state_ref in enumerate((one_ref, two_ref)):
            state = jnp.zeros_like(state_ref)
            first = g * sizes[0]
            for prior in reversed(priors):
                facts = prior[base:].astype(jnp.float32)
                decay = facts[8 * g : 8 * g + 1] + facts[8 * g + 4 : 8 * g + 5]
                own = prior[first : first + sizes[g]].astype(jnp.float32)
                state = state * jnp.exp(decay) + own
            state_ref[...] = state

    bound = 0
    out = []
    for g, (enter_ref, state_ref) in enumerate(((enter_one_ref, one_ref), (enter_two_ref, two_ref))):
        queries = rows_ref[:, bound + sizes[g] : bound + 2 * sizes[g]]
        bound += 2 * sizes[g]
        here = slice(g * lanes, (g + 1) * lanes)
        entering = enter_ref[0] + state_ref[...] * earlier_ref[0:1, here]
        far = jnp.dot(
            queries, entering.astype(jnp.bfloat16), preferred_element_type=jnp.float32
        )
        reach = down_ref[:, 2 * high + g * heads : 2 * high + (g + 1) * heads]
        gate = gate_ref[:, g].astype(jnp.float32)
        total = near_ref[:, here] + far * widened(reach, heads, HEAD_DIM)
        gated = total * (gate * jax.nn.sigmoid(gate))
        squares = gated * gated
        means = jnp.concatenate(
            [
                jnp.sum(squares[:, h * HEAD_DIM : (h + 1) * HEAD_DIM], axis=1, keepdims=True)
                for h in range(heads)
            ],
            axis=1,
        ) * (1.0 / HEAD_DIM)
        scale = widened(lax.rsqrt(means + EPSILON), heads, HEAD_DIM)
        out.append((gated * scale * gain_ref[g : g + 1]).astype(jnp.bfloat16))
    return jnp.concatenate(out, axis=1)


def mixed_kernel(heads, sizes, prior_count, *refs):
    inputs = prior_count + 8
    refs[inputs][...] = mixed_values(heads, sizes, prior_count, refs[:inputs] + refs[inputs + 1 :])


def projected_kernel(heads, sizes, prior_count, turns, order_ref, *refs):
    inputs = prior_count + 8
    matrix_ref, outs = refs[inputs], refs[inputs + 1 : inputs + 1 + turns]
    mixed = mixed_values(heads, sizes, prior_count, refs[:inputs] + refs[inputs + 1 + turns :])
    product = jnp.dot(mixed, matrix_ref[...], preferred_element_type=jnp.float32)
    for turn, out_ref in enumerate(outs):

        @pl.when(pl.program_id(0) == turn)
        def _(out_ref=out_ref):
            out_ref[...] = product.astype(jnp.bfloat16)


def mixed_rows(
    grouped_value_heads,
    output_gate_heads,
    projected_key_query,
    raw_step_size,
    step_size_bias,
    head_decay_logarithm,
    position_extra_decay,
    head_skip_weight,
    value_kernel_taps,
    key_query_kernel,
    head_norm_gain,
    output_matrix,
    order,
):
    positions, _, lanes = grouped_value_heads.shape
    heads = lanes // HEAD_DIM
    high = high_rows(heads)
    sizes = (STATE_ONE, STATE_TWO)
    width = key_query_kernel.shape[1]
    blocks = positions // BLOCK
    last = grouped_value_heads[positions - 8 :].reshape(8, 2 * lanes)
    rim = passed_along(
        jnp.concatenate([last, projected_key_query[positions - 8 :]], axis=1), "sp", 1
    )
    facts = jnp.concatenate([step_size_bias, head_decay_logarithm, head_skip_weight], axis=0)
    steps = raw_step_size.transpose(1, 2, 0)

    def by_block(rows, columns):
        return pl.BlockSpec((rows, columns), lambda k: (k, 0))

    def along(rows):
        return pl.BlockSpec((rows, BLOCK), lambda k: (0, k))

    def fixed(*shape):
        return pl.BlockSpec(shape, lambda k: (0,) * len(shape))

    def per_block(*shape):
        return pl.BlockSpec((1, *shape), lambda k: (k,) + (0,) * len(shape))

    f32, bf16 = jnp.float32, jnp.bfloat16
    packed_rows = sizes[0] + sizes[1] + 16
    x, rows, across, down, enter_one, enter_two, earlier, packed = pl.pallas_call(
        functools.partial(states_kernel, heads, sizes),
        grid=(blocks,),
        in_specs=[
            pl.BlockSpec((BLOCK, 2, lanes), lambda k: (k, 0, 0)),
            by_block(BLOCK, width),
            fixed(8, 2 * lanes + width),
            fixed(*value_kernel_taps.shape),
            fixed(*key_query_kernel.shape),
            pl.BlockSpec((2, heads, BLOCK), lambda k: (0, 0, k)),
            fixed(6, heads),
            along(1),
        ],
        out_specs=[
            by_block(BLOCK, 2 * lanes),
            by_block(BLOCK, width),
            along(2 * high),
            by_block(BLOCK, BLOCK),
            per_block(sizes[0], lanes),
            per_block(sizes[1], lanes),
            by_block(8, 2 * lanes),
            fixed(packed_rows, lanes),
        ],
        out_shape=[
            jax.ShapeDtypeStruct((positions, 2 * lanes), bf16),
            jax.ShapeDtypeStruct((positions, width), bf16),
            jax.ShapeDtypeStruct((2 * high, positions), f32),
            jax.ShapeDtypeStruct((positions, BLOCK), f32),
            jax.ShapeDtypeStruct((blocks, sizes[0], lanes), f32),
            jax.ShapeDtypeStruct((blocks, sizes[1], lanes), f32),
            jax.ShapeDtypeStruct((8 * blocks, 2 * lanes), f32),
            jax.ShapeDtypeStruct((packed_rows, lanes), bf16),
        ],
        scratch_shapes=[
            pltpu.VMEM((8, 2 * lanes + width), f32),
            pltpu.VMEM((sizes[0], lanes), f32),
            pltpu.VMEM((sizes[1], lanes), f32),
            pltpu.VMEM((high, 1), f32),
        ],
        name="states",
    )(
        grouped_value_heads,
        projected_key_query,
        rim,
        value_kernel_taps,
        key_query_kernel,
        steps,
        facts,
        position_extra_decay[None],
    )
    priors = [passed_along(packed, "sp", by) for by in range(1, lax.axis_size("sp"))]
    near = pl.pallas_call(
        functools.partial(near_kernel, heads, sizes),
        grid=(blocks,),
        in_specs=[
            by_block(BLOCK, 2 * lanes),
            by_block(BLOCK, width),
            along(2 * high),
            by_block(BLOCK, BLOCK),
            fixed(6, heads),
        ],
        out_specs=by_block(BLOCK, 2 * lanes),
        out_shape=jax.ShapeDtypeStruct((positions, 2 * lanes), f32),
        name="near",
    )(x, rows, across, down, facts)
    operands = (
        *priors,
        near,
        rows,
        down,
        enter_one,
        enter_two,
        earlier,
        output_gate_heads,
        head_norm_gain,
    )
    scratch_shapes = [pltpu.VMEM((sizes[0], lanes), f32), pltpu.VMEM((sizes[1], lanes), f32)]
    if order is None:
        return pl.pallas_call(
            functools.partial(mixed_kernel, heads, sizes, len(priors)),
            grid=(blocks,),
            in_specs=[fixed(packed_rows, lanes) for _ in priors]
            + [
                by_block(BLOCK, 2 * lanes),
                by_block(BLOCK, width),
                by_block(BLOCK, BLOCK),
                per_block(sizes[0], lanes),
                per_block(sizes[1], lanes),
                by_block(8, 2 * lanes),
                pl.BlockSpec((BLOCK, 2, lanes), lambda k: (k, 0, 0)),
                fixed(2, lanes),
            ],
            out_specs=by_block(BLOCK, 2 * lanes),
            out_shape=jax.ShapeDtypeStruct((positions, 2 * lanes), bf16),
            scratch_shapes=scratch_shapes,
            name="mixed",
        )(*operands)

    def whole(*shape):
        return pl.BlockSpec(shape, lambda k, order: (0,) * len(shape))

    model_width = output_matrix.shape[2]
    outs = {}
    for turns in ((3, 2), (1, 0)):
        count = len(turns)

        def target(k, order, turns=turns):
            return order[0] ^ jnp.where(k == 0, MASKS[turns[0]], MASKS[turns[1]])

        def chosen(rows, columns, target=target):
            return pl.BlockSpec((rows, columns), lambda k, order: (target(k, order), 0))

        def chosen_state(*shape, target=target):
            rest = (0,) * len(shape)
            return pl.BlockSpec((1, *shape), lambda k, order: (target(k, order), *rest))

        results = pl.pallas_call(
            functools.partial(projected_kernel, heads, sizes, len(priors), count),
            grid_spec=pltpu.PrefetchScalarGridSpec(
                num_scalar_prefetch=1,
                grid=(count,),
                in_specs=[whole(packed_rows, lanes) for _ in priors]
                + [
                    chosen(BLOCK, 2 * lanes),
                    chosen(BLOCK, width),
                    chosen(BLOCK, BLOCK),
                    chosen_state(sizes[0], lanes),
                    chosen_state(sizes[1], lanes),
                    chosen(8, 2 * lanes),
                    pl.BlockSpec((BLOCK, 2, lanes), lambda k, order, t=target: (t(k, order), 0, 0)),
                    whole(2, lanes),
                    whole(2 * lanes, model_width),
                ],
                out_specs=[whole(BLOCK, model_width)] * count,
                scratch_shapes=scratch_shapes,
            ),
            out_shape=[jax.ShapeDtypeStruct((BLOCK, model_width), bf16)] * count,
            name="projected",
        )(order[None], *operands, output_matrix.reshape(2 * lanes, model_width))
        outs.update(zip(turns, results))
    return [outs[turn] for turn in range(blocks)]


def routed_experts(
    wide_stream, normed, gate_weight, up_weight, down_weight, token_expert_choice, expert_output_weight
):
    rows_here, model_width = normed.shape
    expert_total = lax.axis_size("sp")
    capacity = 2 * rows_here // expert_total + 1
    flat_ids = token_expert_choice.reshape(-1)
    matches = (flat_ids[:, None] == jnp.arange(expert_total, dtype=jnp.int32)[None, :]).astype(
        jnp.int32
    )
    slot_rank = jnp.sum((jnp.cumsum(matches, axis=0) - matches) * matches, axis=1)
    target = flat_ids * capacity + slot_rank
    outbound = (
        jnp.zeros((expert_total * capacity, model_width), jnp.bfloat16)
        .at[target]
        .set(jnp.repeat(normed, 2, axis=0))
    )
    outbound = outbound.reshape(expert_total, capacity, model_width)
    widened = lax.all_gather(
        lax.all_to_all(outbound, "sp", split_axis=0, concat_axis=0, tiled=True),
        "tp",
        axis=0,
        tiled=True,
    )
    flat_rows = widened.reshape(-1, widened.shape[-1])
    gate_out = jnp.dot(flat_rows, gate_weight, preferred_element_type=jnp.float32)
    up_out = jnp.dot(flat_rows, up_weight, preferred_element_type=jnp.float32)
    hidden = (jax.nn.silu(gate_out) * up_out).astype(jnp.bfloat16)
    partial_value = jnp.dot(
        hidden, down_weight, preferred_element_type=jnp.float32
    ).astype(jnp.bfloat16)
    partial_value = lax.optimization_barrier(
        partial_value.reshape(widened.shape[0], widened.shape[1], partial_value.shape[-1])
    ).astype(jnp.float32)
    summed = lax.psum_scatter(
        partial_value.astype(jnp.bfloat16), "tp", scatter_dimension=0, tiled=True
    )
    returned = lax.all_to_all(summed, "sp", split_axis=0, concat_axis=0, tiled=True)
    picked = jnp.take(returned.reshape(expert_total * capacity, model_width), target, axis=0)
    picked = picked.reshape(rows_here, 2, model_width).astype(jnp.float32)
    weighted = (
        expert_output_weight[:, 0:1] * picked[:, 0] + expert_output_weight[:, 1:2] * picked[:, 1]
    )
    return (wide_stream + weighted).astype(jnp.bfloat16)


def swapped(array, bit):
    return lax.ppermute(array, "sp", [(i, i ^ bit) for i in range(lax.axis_size("sp"))])


def expert_kernel(region, own_ref, *refs):
    count = len(refs) - 9
    blocks = refs[:count]
    keep_ref, send_ref = refs[count + 3 : count + 5]
    gate_ref, up_ref, back_ref, arrived = refs[count + 5 :]
    fetches = [
        pltpu.make_async_copy(source, target, arrived.at[i])
        for i, (source, target) in enumerate(zip(refs[count : count + 3], (gate_ref, up_ref, back_ref)))
    ]
    for fetch in fetches:
        fetch.start()
    width = gate_ref.shape[0]
    rows = blocks[0].shape[0]
    own = own_ref[0].astype(jnp.float32)
    place = lax.broadcasted_iota(jnp.int32, (region, rows), 0).astype(jnp.float32)
    before = (
        lax.broadcasted_iota(jnp.int32, (rows, rows), 0)
        < lax.broadcasted_iota(jnp.int32, (rows, rows), 1)
    ).astype(jnp.float32)
    named, weights = [], []
    for block in blocks:
        facts = block[:, width:].astype(jnp.float32).T
        hits = (facts[0:2] == own).astype(jnp.float32)
        named.append(hits[0:1] + hits[1:2])
        weights.append(
            hits[0:1] * (facts[2:3] + facts[4:5]) + hits[1:2] * (facts[3:4] + facts[5:6])
        )
    named = jnp.concatenate(named + named[: max(8 - count, 0)], axis=0)
    inner = jnp.dot(named, before, preferred_element_type=jnp.float32)
    slot = jnp.where(named > 0, inner, -1.0)
    taken = []
    for i, block in enumerate(blocks):
        chosen = (place == slot[i : i + 1]).astype(jnp.bfloat16)
        taken.append(jnp.dot(chosen, block[:, :width], preferred_element_type=jnp.float32))
    taken = jnp.concatenate(taken, axis=0).astype(jnp.bfloat16)
    down = jnp.concatenate(
        [slot[0:count]] + weights + [jnp.zeros((rows - 2 * count, rows), jnp.float32)], axis=0
    ).T
    fetches[0].wait()
    gate = jnp.dot(taken, gate_ref[...], preferred_element_type=jnp.float32)
    fetches[1].wait()
    up = jnp.dot(taken, up_ref[...], preferred_element_type=jnp.float32)
    hidden = (gate * jax.nn.sigmoid(gate) * up).astype(jnp.bfloat16)
    fetches[2].wait()
    result = jnp.dot(hidden, back_ref[...], preferred_element_type=jnp.float32)
    place = lax.broadcasted_iota(jnp.int32, (rows, region), 1).astype(jnp.float32)
    for i in range(count):
        chosen = (place == down[:, i : i + 1]).astype(jnp.bfloat16)
        spread = jnp.dot(
            chosen,
            result[i * region : (i + 1) * region].astype(jnp.bfloat16),
            preferred_element_type=jnp.float32,
        )
        out_ref = (keep_ref, send_ref)[2 * i // count]
        first = i % (count // 2) * rows
        out_ref[first : first + rows] = (
            spread * down[:, count + i : count + i + 1]
        ).astype(jnp.bfloat16)


def run_expert(blocks, own, gate_weight, up_weight, down_weight, capacity):
    rows = blocks[0].shape[0]
    width, hidden = gate_weight.shape
    region = -(-capacity // 8) * 8
    vmem = pl.BlockSpec(memory_space=pltpu.VMEM)
    return pl.pallas_call(
        functools.partial(expert_kernel, region),
        in_specs=[pl.BlockSpec(memory_space=pltpu.SMEM)]
        + [vmem] * len(blocks)
        + [pl.BlockSpec(memory_space=pl.ANY)] * 3,
        out_specs=[vmem] * 2,
        out_shape=[jax.ShapeDtypeStruct((len(blocks) // 2 * rows, width), jnp.bfloat16)] * 2,
        scratch_shapes=[
            pltpu.VMEM((width, hidden), jnp.bfloat16),
            pltpu.VMEM((width, hidden), jnp.bfloat16),
            pltpu.VMEM((hidden, width), jnp.bfloat16),
            pltpu.SemaphoreType.DMA((3,)),
        ],
        cost_estimate=pl.CostEstimate(
            flops=6 * len(blocks) * region * width * hidden,
            bytes_accessed=6 * width * hidden,
            transcendentals=len(blocks) * region * hidden,
        ),
        name="expert",
    )(own[None], *blocks, gate_weight, up_weight, down_weight)


def added(block, *received):
    if len(received) == 1:
        return block + received[0]
    total = block.astype(jnp.float32)
    for other in received:
        if other is not None:
            total = total + other.astype(jnp.float32)
    return total.astype(jnp.bfloat16)


def stream_kernel(
    residual_ref, own_ref, one_ref, two_ref, three_ref, gain_ref, facts_ref, stream_ref, rows_ref
):
    total = own_ref[...].astype(jnp.float32) + residual_ref[...].astype(jnp.float32)
    for ref in (one_ref, two_ref, three_ref):
        total = total + ref[...].astype(jnp.float32)
    stream = total.astype(jnp.bfloat16)
    stream_ref[...] = stream
    wide = stream.astype(jnp.float32)
    scale = lax.rsqrt(jnp.mean(wide * wide, axis=1, keepdims=True) + EPSILON)
    width = wide.shape[1]
    rows_ref[:, :width] = (wide * scale * gain_ref[...]).astype(jnp.bfloat16)
    rows_ref[:, width:] = facts_ref[...]


def stream_and_rows(residual, parts, gain, token_expert_choice, expert_output_weight):
    rows, width = residual.shape
    high = expert_output_weight.astype(jnp.bfloat16)
    low = (expert_output_weight - high.astype(jnp.float32)).astype(jnp.bfloat16)
    facts = jnp.concatenate([token_expert_choice.astype(jnp.bfloat16), high, low], axis=1)
    facts = jnp.pad(facts, ((0, 0), (0, rows - facts.shape[1])))
    return pl.pallas_call(
        stream_kernel,
        out_shape=[
            jax.ShapeDtypeStruct((rows, width), jnp.bfloat16),
            jax.ShapeDtypeStruct((rows, width + rows), jnp.bfloat16),
        ],
        name="stream",
    )(residual, *parts, gain[None], facts)


SWAPS = [(0, 1), (1, 0), (2, 3), (3, 2)]
MIDDLE = [(1, 2), (2, 1)]
ENDS = [(0, 3), (3, 0)]
OUTWARD = [(1, 0), (2, 3)]
INWARD = [(0, 1), (3, 2)]
MASKS = (0, 1, 3, 2)


def line_sum(parts):
    ends = lax.ppermute(parts[2], "tp", ENDS)
    middle = lax.ppermute(parts[3], "tp", MIDDLE)
    inward = lax.ppermute(parts[3], "tp", INWARD)
    pair = lax.ppermute(added(parts[1], middle), "tp", SWAPS)
    middle_two = lax.ppermute(added(parts[2], inward), "tp", MIDDLE)
    return parts[0], ends, pair, middle_two


def final_kernel(stream_ref, *refs):
    out_ref = refs[-1]
    total = stream_ref[...].astype(jnp.float32)
    for ref in refs[:-1]:
        total = total + ref[...].astype(jnp.float32)
    out_ref[...] = total.astype(jnp.bfloat16)


def near_kernel_sum(keep_ref, back_ref, out_ref):
    total = keep_ref[...].astype(jnp.float32) + back_ref[...].astype(jnp.float32)
    out_ref[...] = total.astype(jnp.bfloat16)


def near_added(keep, back):
    rows, width = keep.shape
    half = pl.BlockSpec((rows // 2, width), lambda k: (0, 0))
    return pl.pallas_call(
        near_kernel_sum,
        grid=(1,),
        in_specs=[half, half],
        out_specs=half,
        out_shape=jax.ShapeDtypeStruct((rows // 2, width), jnp.bfloat16),
        name="near_sum",
    )(keep, back)


def dense_experts(stream, normed, gate_weight, up_weight, down_weight):
    rows = normed.shape[0]
    capacity = 2 * rows // lax.axis_size("sp") + 1
    place = lax.axis_index("tp")
    mine = lax.axis_index("sp").astype(jnp.int32)
    inner = (place == 1) | (place == 2)

    far = [swapped(normed, 2)]
    from_pair = lax.ppermute(normed, "tp", SWAPS)
    second = lax.ppermute(normed, "tp", MIDDLE + ENDS)
    middle_two = lax.ppermute(from_pair, "tp", MIDDLE)
    outer_two = lax.ppermute(second, "tp", OUTWARD)
    third = jnp.where(inner, middle_two, outer_two)
    blocks = [normed, from_pair, second, third]
    sums = []
    near_other, far_other = [], []
    for turn in range(4):
        if turn:
            far.append(swapped(blocks[turn], 2))
        near_other.append(swapped(blocks[turn], 1))
        far_other.append(swapped(far[turn], 1))
    experts = (mine, gate_weight, up_weight, down_weight, capacity)
    near, crossed = [], []
    for turns in ((0, 1), (2,), (3,)):
        kept = [b for turn in turns for b in (blocks[turn], far[turn])]
        sent = [b for turn in turns for b in (near_other[turn], far_other[turn])]
        keep, send = run_expert(kept + sent, *experts)
        back = swapped(send, 1)
        fenced = lax.optimization_barrier((keep, back))
        for i, turn in enumerate(turns):
            here = slice(2 * i * rows, (2 * i + 1) * rows)
            beyond = slice((2 * i + 1) * rows, 2 * (i + 1) * rows)
            near.append((fenced[0][here], fenced[1][here]))
            crossed.append(swapped(added(keep[beyond], back[beyond]), 2))
    near_last = near_added(keep, back)
    parts = [None]
    for turn in (1, 2):
        parts.append(added(*near[turn], crossed[turn]))
    parts[2] = lax.optimization_barrier(parts[2])
    parts.append(lax.optimization_barrier(added(near_last, crossed[3])))
    sums = line_sum(parts)[1:]
    return pl.pallas_call(
        final_kernel,
        out_shape=jax.ShapeDtypeStruct(stream.shape, jnp.bfloat16),
        name="final",
    )(stream, *near[0], crossed[0], *sums)


def local(
    residual,
    grouped_value_heads,
    output_gate_heads,
    projected_key_query,
    raw_step_size,
    step_size_bias,
    head_decay_logarithm,
    position_extra_decay,
    head_skip_weight,
    value_kernel_taps,
    key_query_kernel,
    head_norm_gain,
    output_matrix,
    expert_norm_gain,
    expert_gate_weight,
    expert_up_weight,
    expert_down_weight,
    token_expert_choice,
    expert_output_weight,
):
    lane_width = grouped_value_heads.shape[2]
    dense = lax.axis_size("sp") == 4 and lax.axis_size("tp") == 4
    order = lax.axis_index("tp").astype(jnp.int32) if dense else None
    mixed_heads = mixed_rows(
        grouped_value_heads,
        output_gate_heads,
        projected_key_query,
        raw_step_size,
        step_size_bias,
        head_decay_logarithm,
        position_extra_decay,
        head_skip_weight,
        value_kernel_taps,
        key_query_kernel,
        head_norm_gain,
        output_matrix,
        order,
    )
    weights = (expert_gate_weight[0], expert_up_weight[0], expert_down_weight[0])
    if dense:
        stream, normed = stream_and_rows(
            residual,
            line_sum(mixed_heads),
            expert_norm_gain,
            token_expert_choice,
            expert_output_weight,
        )
        return dense_experts(stream, normed, *weights)
    model_width = output_matrix.shape[2]
    mix_out = lax.psum_scatter(
        jnp.dot(
            mixed_heads,
            output_matrix.reshape(2 * lane_width, model_width),
            preferred_element_type=jnp.float32,
        ).astype(jnp.bfloat16),
        "tp",
        scatter_dimension=0,
        tiled=True,
    ).astype(jnp.float32)
    stream = (residual.astype(jnp.float32) + mix_out).astype(jnp.bfloat16)
    wide_stream = stream.astype(jnp.float32)
    normed = (
        wide_stream
        * lax.rsqrt(jnp.mean(wide_stream * wide_stream, axis=1, keepdims=True) + EPSILON)
        * expert_norm_gain[None]
    ).astype(jnp.bfloat16)
    return routed_experts(wide_stream, normed, *weights, token_expert_choice, expert_output_weight)


def solution(mesh):
    placed = (
        P(("grp", "sp", "tp"), None),
        P(("grp", "sp"), None, "tp"),
        P(("grp", "sp"), None, "tp"),
        P(("grp", "sp"), None),
        P(("grp", "sp"), None, "tp"),
        P(None, "tp"),
        P(None, "tp"),
        P(("grp", "sp")),
        P(None, "tp"),
        P(None, None, "tp"),
        P(),
        P(None, "tp"),
        P(None, "tp", None),
        P(),
        P("sp", None, "tp"),
        P("sp", None, "tp"),
        P("sp", "tp", None),
        P(("grp", "sp", "tp"), None),
        P(("grp", "sp", "tp"), None),
    )

    return jax.shard_map(
        local, mesh=mesh, in_specs=placed, out_specs=P(("grp", "sp", "tp"), None), check_vma=False
    )
```

```python
import functools

import jax
import jax.numpy as jnp
from jax import lax
from jax.experimental import pallas as pl
from jax.experimental.pallas import tpu as pltpu
from jax.sharding import PartitionSpec as P


HEAD_DIM = 64
STATE_ONE = 64
STATE_TWO = 128
BLOCK = 128


EPSILON = 1e-06


def passed_along(shard, axis, by):
    length = lax.axis_size(axis)
    pairs = [(i, i + by) for i in range(length) if 0 <= i + by < length]
    return lax.ppermute(shard, axis, pairs)


def high_rows(heads):
    return -(-2 * heads // 8) * 8


def widened(column, heads, width):
    rows = column.shape[0]
    return jnp.concatenate(
        [jnp.broadcast_to(column[:, h : h + 1], (rows, width)) for h in range(heads)], axis=1
    )


def spread_down(tall, first, heads, width):
    return jnp.concatenate(
        [jnp.broadcast_to(tall[first + h : first + h + 1], (1, width)) for h in range(heads)], axis=1
    )


def both_groups(tall, heads, width):
    return jnp.concatenate(
        [spread_down(tall, g * heads, heads, width) for g in range(2)], axis=1
    )


def head_facts(facts_ref, kind, high):
    heads = facts_ref.shape[1]
    both = jnp.concatenate(
        [facts_ref[2 * kind : 2 * kind + 1], facts_ref[2 * kind + 1 : 2 * kind + 2]], axis=1
    )
    if high > 2 * heads:
        both = jnp.concatenate([both, jnp.zeros((1, high - 2 * heads), jnp.float32)], axis=1)
    same = lax.broadcasted_iota(jnp.int32, (high, high), 0) == lax.broadcasted_iota(
        jnp.int32, (high, high), 1
    )
    return jnp.sum(jnp.where(same, jnp.broadcast_to(both, (high, high)), 0.0), axis=1, keepdims=True)


def states_kernel(
    heads,
    sizes,
    values_ref,
    keys_ref,
    rim_ref,
    value_taps_ref,
    key_taps_ref,
    steps_ref,
    facts_ref,
    extra_ref,
    x_ref,
    rows_ref,
    across_ref,
    down_ref,
    enter_one_ref,
    enter_two_ref,
    earlier_ref,
    packed_ref,
    tail_ref,
    one_ref,
    two_ref,
    sum_ref,
):
    step = pl.program_id(0)
    lanes = heads * HEAD_DIM
    taps = value_taps_ref.shape[0]

    @pl.when(step == 0)
    def _():
        tail_ref[...] = rim_ref[...].astype(jnp.float32)
        one_ref[...] = jnp.zeros_like(one_ref)
        two_ref[...] = jnp.zeros_like(two_ref)
        sum_ref[...] = jnp.zeros_like(sum_ref)

    here = jnp.concatenate(
        [values_ref[:, g].astype(jnp.float32) for g in range(2)]
        + [keys_ref[...].astype(jnp.float32)],
        axis=1,
    )
    extended = jnp.concatenate([tail_ref[...], here], axis=0)
    tail_ref[...] = here[BLOCK - 8 :]
    weights = jnp.concatenate(
        [value_taps_ref[:, g].astype(jnp.float32) for g in range(2)]
        + [key_taps_ref[...].astype(jnp.float32)],
        axis=1,
    )
    summed = jnp.zeros_like(here)
    for j in range(taps):
        first = 8 - (taps - 1) + j
        summed = summed + extended[first : first + BLOCK] * weights[j : j + 1]
    active = (summed * jax.nn.sigmoid(summed)).astype(jnp.bfloat16)
    x = active[:, : 2 * lanes]
    rows = active[:, 2 * lanes :]
    x_ref[...] = x
    rows_ref[...] = rows

    high = high_rows(heads)
    raw = [steps_ref[g].astype(jnp.float32) for g in range(2)]
    if high > 2 * heads:
        raw.append(jnp.zeros((high - 2 * heads, BLOCK), jnp.float32))
    raw = jnp.concatenate(raw, axis=0) + head_facts(facts_ref, 0, high)
    stride = jnp.maximum(raw, 0.0) + jnp.log1p(jnp.exp(-jnp.abs(raw)))
    log_decay = extra_ref[...] - jnp.exp(head_facts(facts_ref, 1, high)) * stride
    upto = (
        lax.broadcasted_iota(jnp.int32, (BLOCK, BLOCK), 0)
        <= lax.broadcasted_iota(jnp.int32, (BLOCK, BLOCK), 1)
    ).astype(jnp.float32)
    running = jnp.dot(
        log_decay, upto, preferred_element_type=jnp.float32, precision=lax.Precision.HIGHEST
    )
    end = running[:, BLOCK - 1 :]
    fading = jnp.exp(end - running) * stride
    stacked = jnp.concatenate(
        [running, fading, jnp.exp(running)]
        + [jnp.zeros((BLOCK - 3 * high, BLOCK), jnp.float32)],
        axis=0,
    )
    down = stacked.T
    across_ref[...] = jnp.concatenate([running, stride], axis=0)
    down_ref[...] = down
    earlier_ref[...] = jnp.broadcast_to(
        jnp.exp(both_groups(sum_ref[...], heads, HEAD_DIM)), earlier_ref.shape
    )
    faded_end = jnp.exp(both_groups(end, heads, HEAD_DIM))
    bound = 0
    for g, (enter_ref, state_ref) in enumerate(((enter_one_ref, one_ref), (enter_two_ref, two_ref))):
        keys = rows[:, bound : bound + sizes[g]]
        bound += 2 * sizes[g]
        fade = widened(down[:, high + g * heads : high + (g + 1) * heads], heads, HEAD_DIM)
        scaled = (x[:, g * lanes : (g + 1) * lanes].astype(jnp.float32) * fade).astype(jnp.bfloat16)
        own = lax.dot_general(
            keys, scaled, (((0,), (0,)), ((), ())), preferred_element_type=jnp.float32
        )
        state = state_ref[...]
        enter_ref[0] = state
        state_ref[...] = state * faded_end[:, g * lanes : (g + 1) * lanes] + own
    total = sum_ref[...] + end
    sum_ref[...] = total

    @pl.when(step == pl.num_programs(0) - 1)
    def _():
        whole = both_groups(total, heads, HEAD_DIM)
        high_part = whole.astype(jnp.bfloat16)
        low_part = (whole - high_part.astype(jnp.float32)).astype(jnp.bfloat16)
        packed_ref[0 : sizes[0]] = one_ref[...].astype(jnp.bfloat16)
        packed_ref[sizes[0] : sizes[0] + sizes[1]] = two_ref[...].astype(jnp.bfloat16)
        packed_ref[sizes[0] + sizes[1] :] = jnp.concatenate(
            [
                jnp.broadcast_to(part[:, g * lanes : (g + 1) * lanes].astype(jnp.float32), (4, lanes))
                for g in range(2)
                for part in (high_part, low_part)
            ],
            axis=0,
        ).astype(jnp.bfloat16)


def near_kernel(heads, sizes, x_ref, rows_ref, across_ref, down_ref, facts_ref, near_ref):
    high = across_ref.shape[0] // 2
    later = lax.broadcasted_iota(jnp.int32, (BLOCK, BLOCK), 0) >= lax.broadcasted_iota(
        jnp.int32, (BLOCK, BLOCK), 1
    )
    skip = both_groups(head_facts(facts_ref, 2, high), heads, HEAD_DIM)
    bound = 0
    out = []
    for g in range(2):
        keys = rows_ref[:, bound : bound + sizes[g]]
        queries = rows_ref[:, bound + sizes[g] : bound + 2 * sizes[g]]
        bound += 2 * sizes[g]
        scores = lax.dot_general(
            queries, keys, (((1,), (1,)), ((), ())), preferred_element_type=jnp.float32
        )
        for h in range(heads):
            i = g * heads + h
            spread = jnp.where(later, down_ref[:, i : i + 1] - across_ref[i : i + 1], -1e30)
            weights = scores * jnp.exp(spread) * across_ref[high + i : high + i + 1]
            x = x_ref[:, i * HEAD_DIM : (i + 1) * HEAD_DIM]
            out.append(
                jnp.dot(weights.astype(jnp.bfloat16), x, preferred_element_type=jnp.float32)
            )
    near_ref[...] = jnp.concatenate(out, axis=1) + skip * x_ref[...].astype(jnp.float32)


def mixed_values(heads, sizes, prior_count, refs):
    priors = refs[:prior_count]
    (
        near_ref,
        rows_ref,
        down_ref,
        enter_one_ref,
        enter_two_ref,
        earlier_ref,
        gate_ref,
        gain_ref,
        one_ref,
        two_ref,
    ) = refs[prior_count:]
    lanes = heads * HEAD_DIM
    high = high_rows(heads)

    @pl.when(pl.program_id(0) == 0)
    def _():
        base = sizes[0] + sizes[1]
        for g, state_ref in enumerate((one_ref, two_ref)):
            state = jnp.zeros_like(state_ref)
            first = g * sizes[0]
            for prior in reversed(priors):
                facts = prior[base:].astype(jnp.float32)
                decay = facts[8 * g : 8 * g + 1] + facts[8 * g + 4 : 8 * g + 5]
                own = prior[first : first + sizes[g]].astype(jnp.float32)
                state = state * jnp.exp(decay) + own
            state_ref[...] = state

    bound = 0
    out = []
    for g, (enter_ref, state_ref) in enumerate(((enter_one_ref, one_ref), (enter_two_ref, two_ref))):
        queries = rows_ref[:, bound + sizes[g] : bound + 2 * sizes[g]]
        bound += 2 * sizes[g]
        here = slice(g * lanes, (g + 1) * lanes)
        entering = enter_ref[0] + state_ref[...] * earlier_ref[0:1, here]
        far = jnp.dot(
            queries, entering.astype(jnp.bfloat16), preferred_element_type=jnp.float32
        )
        reach = down_ref[:, 2 * high + g * heads : 2 * high + (g + 1) * heads]
        gate = gate_ref[:, g].astype(jnp.float32)
        total = near_ref[:, here] + far * widened(reach, heads, HEAD_DIM)
        gated = total * (gate * jax.nn.sigmoid(gate))
        squares = gated * gated
        means = jnp.concatenate(
            [
                jnp.sum(squares[:, h * HEAD_DIM : (h + 1) * HEAD_DIM], axis=1, keepdims=True)
                for h in range(heads)
            ],
            axis=1,
        ) * (1.0 / HEAD_DIM)
        scale = widened(lax.rsqrt(means + EPSILON), heads, HEAD_DIM)
        out.append((gated * scale * gain_ref[g : g + 1]).astype(jnp.bfloat16))
    return jnp.concatenate(out, axis=1)


def mixed_kernel(heads, sizes, prior_count, *refs):
    inputs = prior_count + 8
    refs[inputs][...] = mixed_values(heads, sizes, prior_count, refs[:inputs] + refs[inputs + 1 :])


def projected_kernel(heads, sizes, prior_count, turns, order_ref, *refs):
    inputs = prior_count + 8
    matrix_ref, outs = refs[inputs], refs[inputs + 1 : inputs + 1 + turns]
    mixed = mixed_values(heads, sizes, prior_count, refs[:inputs] + refs[inputs + 1 + turns :])
    product = jnp.dot(mixed, matrix_ref[...], preferred_element_type=jnp.float32)
    for turn, out_ref in enumerate(outs):

        @pl.when(pl.program_id(0) == turn)
        def _(out_ref=out_ref):
            out_ref[...] = product.astype(jnp.bfloat16)


def mixed_rows(
    grouped_value_heads,
    output_gate_heads,
    projected_key_query,
    raw_step_size,
    step_size_bias,
    head_decay_logarithm,
    position_extra_decay,
    head_skip_weight,
    value_kernel_taps,
    key_query_kernel,
    head_norm_gain,
    output_matrix,
    order,
):
    positions, _, lanes = grouped_value_heads.shape
    heads = lanes // HEAD_DIM
    high = high_rows(heads)
    sizes = (STATE_ONE, STATE_TWO)
    width = key_query_kernel.shape[1]
    blocks = positions // BLOCK
    last = grouped_value_heads[positions - 8 :].reshape(8, 2 * lanes)
    rim = passed_along(
        jnp.concatenate([last, projected_key_query[positions - 8 :]], axis=1), "sp", 1
    )
    facts = jnp.concatenate([step_size_bias, head_decay_logarithm, head_skip_weight], axis=0)
    steps = raw_step_size.transpose(1, 2, 0)

    def by_block(rows, columns):
        return pl.BlockSpec((rows, columns), lambda k: (k, 0))

    def along(rows):
        return pl.BlockSpec((rows, BLOCK), lambda k: (0, k))

    def fixed(*shape):
        return pl.BlockSpec(shape, lambda k: (0,) * len(shape))

    def per_block(*shape):
        return pl.BlockSpec((1, *shape), lambda k: (k,) + (0,) * len(shape))

    f32, bf16 = jnp.float32, jnp.bfloat16
    packed_rows = sizes[0] + sizes[1] + 16
    x, rows, across, down, enter_one, enter_two, earlier, packed = pl.pallas_call(
        functools.partial(states_kernel, heads, sizes),
        grid=(blocks,),
        in_specs=[
            pl.BlockSpec((BLOCK, 2, lanes), lambda k: (k, 0, 0)),
            by_block(BLOCK, width),
            fixed(8, 2 * lanes + width),
            fixed(*value_kernel_taps.shape),
            fixed(*key_query_kernel.shape),
            pl.BlockSpec((2, heads, BLOCK), lambda k: (0, 0, k)),
            fixed(6, heads),
            along(1),
        ],
        out_specs=[
            by_block(BLOCK, 2 * lanes),
            by_block(BLOCK, width),
            along(2 * high),
            by_block(BLOCK, BLOCK),
            per_block(sizes[0], lanes),
            per_block(sizes[1], lanes),
            by_block(8, 2 * lanes),
            fixed(packed_rows, lanes),
        ],
        out_shape=[
            jax.ShapeDtypeStruct((positions, 2 * lanes), bf16),
            jax.ShapeDtypeStruct((positions, width), bf16),
            jax.ShapeDtypeStruct((2 * high, positions), f32),
            jax.ShapeDtypeStruct((positions, BLOCK), f32),
            jax.ShapeDtypeStruct((blocks, sizes[0], lanes), f32),
            jax.ShapeDtypeStruct((blocks, sizes[1], lanes), f32),
            jax.ShapeDtypeStruct((8 * blocks, 2 * lanes), f32),
            jax.ShapeDtypeStruct((packed_rows, lanes), bf16),
        ],
        scratch_shapes=[
            pltpu.VMEM((8, 2 * lanes + width), f32),
            pltpu.VMEM((sizes[0], lanes), f32),
            pltpu.VMEM((sizes[1], lanes), f32),
            pltpu.VMEM((high, 1), f32),
        ],
        name="states",
    )(
        grouped_value_heads,
        projected_key_query,
        rim,
        value_kernel_taps,
        key_query_kernel,
        steps,
        facts,
        position_extra_decay[None],
    )
    priors = [passed_along(packed, "sp", by) for by in range(1, lax.axis_size("sp"))]
    near_sizes = functools.partial(near_kernel, heads, sizes)
    near_operands = (x, rows, across, down, facts)
    operands = (
        rows,
        down,
        enter_one,
        enter_two,
        earlier,
        output_gate_heads,
        head_norm_gain,
    )
    scratch_shapes = [pltpu.VMEM((sizes[0], lanes), f32), pltpu.VMEM((sizes[1], lanes), f32)]
    if order is None:
        near = pl.pallas_call(
            near_sizes,
            grid=(blocks,),
            in_specs=[
                by_block(BLOCK, 2 * lanes),
                by_block(BLOCK, width),
                along(2 * high),
                by_block(BLOCK, BLOCK),
                fixed(6, heads),
            ],
            out_specs=by_block(BLOCK, 2 * lanes),
            out_shape=jax.ShapeDtypeStruct((positions, 2 * lanes), f32),
            name="near",
        )(*near_operands)
        return pl.pallas_call(
            functools.partial(mixed_kernel, heads, sizes, len(priors)),
            grid=(blocks,),
            in_specs=[fixed(packed_rows, lanes) for _ in priors]
            + [
                by_block(BLOCK, 2 * lanes),
                by_block(BLOCK, width),
                by_block(BLOCK, BLOCK),
                per_block(sizes[0], lanes),
                per_block(sizes[1], lanes),
                by_block(8, 2 * lanes),
                pl.BlockSpec((BLOCK, 2, lanes), lambda k: (k, 0, 0)),
                fixed(2, lanes),
            ],
            out_specs=by_block(BLOCK, 2 * lanes),
            out_shape=jax.ShapeDtypeStruct((positions, 2 * lanes), bf16),
            scratch_shapes=scratch_shapes,
            name="mixed",
        )(*priors, near, *operands)

    def whole(*shape):
        return pl.BlockSpec(shape, lambda k, order: (0,) * len(shape))

    model_width = output_matrix.shape[2]
    outs = {}
    for turns in ((3, 2), (1, 0)):
        count = len(turns)

        def target(k, order, turns=turns):
            return order[0] ^ jnp.where(k == 0, MASKS[turns[0]], MASKS[turns[1]])

        def chosen(rows, columns, target=target):
            return pl.BlockSpec((rows, columns), lambda k, order: (target(k, order), 0))

        def chosen_state(*shape, target=target):
            rest = (0,) * len(shape)
            return pl.BlockSpec((1, *shape), lambda k, order: (target(k, order), *rest))

        near = pl.pallas_call(
            lambda order_ref, *refs: near_sizes(*refs),
            grid_spec=pltpu.PrefetchScalarGridSpec(
                num_scalar_prefetch=1,
                grid=(count,),
                in_specs=[
                    chosen(BLOCK, 2 * lanes),
                    chosen(BLOCK, width),
                    pl.BlockSpec((2 * high, BLOCK), lambda k, order, t=target: (0, t(k, order))),
                    chosen(BLOCK, BLOCK),
                    whole(6, heads),
                ],
                out_specs=pl.BlockSpec((BLOCK, 2 * lanes), lambda k, order: (k, 0)),
            ),
            out_shape=jax.ShapeDtypeStruct((count * BLOCK, 2 * lanes), f32),
            name="near",
        )(order[None], *near_operands)
        results = pl.pallas_call(
            functools.partial(projected_kernel, heads, sizes, len(priors), count),
            grid_spec=pltpu.PrefetchScalarGridSpec(
                num_scalar_prefetch=1,
                grid=(count,),
                in_specs=[whole(packed_rows, lanes) for _ in priors]
                + [
                    pl.BlockSpec((BLOCK, 2 * lanes), lambda k, order: (k, 0)),
                    chosen(BLOCK, width),
                    chosen(BLOCK, BLOCK),
                    chosen_state(sizes[0], lanes),
                    chosen_state(sizes[1], lanes),
                    chosen(8, 2 * lanes),
                    pl.BlockSpec((BLOCK, 2, lanes), lambda k, order, t=target: (t(k, order), 0, 0)),
                    whole(2, lanes),
                    whole(2 * lanes, model_width),
                ],
                out_specs=[whole(BLOCK, model_width)] * count,
                scratch_shapes=scratch_shapes,
            ),
            out_shape=[jax.ShapeDtypeStruct((BLOCK, model_width), bf16)] * count,
            name="projected",
        )(order[None], *priors, near, *operands, output_matrix.reshape(2 * lanes, model_width))
        outs.update(zip(turns, results))
    return [outs[turn] for turn in range(blocks)]


def routed_experts(
    wide_stream, normed, gate_weight, up_weight, down_weight, token_expert_choice, expert_output_weight
):
    rows_here, model_width = normed.shape
    expert_total = lax.axis_size("sp")
    capacity = 2 * rows_here // expert_total + 1
    flat_ids = token_expert_choice.reshape(-1)
    matches = (flat_ids[:, None] == jnp.arange(expert_total, dtype=jnp.int32)[None, :]).astype(
        jnp.int32
    )
    slot_rank = jnp.sum((jnp.cumsum(matches, axis=0) - matches) * matches, axis=1)
    target = flat_ids * capacity + slot_rank
    outbound = (
        jnp.zeros((expert_total * capacity, model_width), jnp.bfloat16)
        .at[target]
        .set(jnp.repeat(normed, 2, axis=0))
    )
    outbound = outbound.reshape(expert_total, capacity, model_width)
    widened = lax.all_gather(
        lax.all_to_all(outbound, "sp", split_axis=0, concat_axis=0, tiled=True),
        "tp",
        axis=0,
        tiled=True,
    )
    flat_rows = widened.reshape(-1, widened.shape[-1])
    gate_out = jnp.dot(flat_rows, gate_weight, preferred_element_type=jnp.float32)
    up_out = jnp.dot(flat_rows, up_weight, preferred_element_type=jnp.float32)
    hidden = (jax.nn.silu(gate_out) * up_out).astype(jnp.bfloat16)
    partial_value = jnp.dot(
        hidden, down_weight, preferred_element_type=jnp.float32
    ).astype(jnp.bfloat16)
    partial_value = lax.optimization_barrier(
        partial_value.reshape(widened.shape[0], widened.shape[1], partial_value.shape[-1])
    ).astype(jnp.float32)
    summed = lax.psum_scatter(
        partial_value.astype(jnp.bfloat16), "tp", scatter_dimension=0, tiled=True
    )
    returned = lax.all_to_all(summed, "sp", split_axis=0, concat_axis=0, tiled=True)
    picked = jnp.take(returned.reshape(expert_total * capacity, model_width), target, axis=0)
    picked = picked.reshape(rows_here, 2, model_width).astype(jnp.float32)
    weighted = (
        expert_output_weight[:, 0:1] * picked[:, 0] + expert_output_weight[:, 1:2] * picked[:, 1]
    )
    return (wide_stream + weighted).astype(jnp.bfloat16)


def swapped(array, bit):
    return lax.ppermute(array, "sp", [(i, i ^ bit) for i in range(lax.axis_size("sp"))])


def expert_kernel(region, own_ref, *refs):
    count = (len(refs) - 7) // 2
    blocks = refs[:count]
    outs = refs[count + 3 : 2 * count + 3]
    gate_ref, up_ref, back_ref, arrived = refs[2 * count + 3 :]
    fetches = [
        pltpu.make_async_copy(source, target, arrived.at[i])
        for i, (source, target) in enumerate(zip(refs[count : count + 3], (gate_ref, up_ref, back_ref)))
    ]
    for fetch in fetches:
        fetch.start()
    width = gate_ref.shape[0]
    rows = blocks[0].shape[0]
    own = own_ref[0].astype(jnp.float32)
    place = lax.broadcasted_iota(jnp.int32, (region, rows), 0).astype(jnp.float32)
    before = (
        lax.broadcasted_iota(jnp.int32, (rows, rows), 0)
        < lax.broadcasted_iota(jnp.int32, (rows, rows), 1)
    ).astype(jnp.float32)
    named, weights = [], []
    for block in blocks:
        facts = block[:, width:].astype(jnp.float32).T
        hits = (facts[0:2] == own).astype(jnp.float32)
        named.append(hits[0:1] + hits[1:2])
        weights.append(
            hits[0:1] * (facts[2:3] + facts[4:5]) + hits[1:2] * (facts[3:4] + facts[5:6])
        )
    named = jnp.concatenate(named + named[: max(8 - count, 0)], axis=0)
    inner = jnp.dot(named, before, preferred_element_type=jnp.float32)
    slot = jnp.where(named > 0, inner, -1.0)
    taken = []
    for i, block in enumerate(blocks):
        chosen = (place == slot[i : i + 1]).astype(jnp.bfloat16)
        taken.append(jnp.dot(chosen, block[:, :width], preferred_element_type=jnp.float32))
    taken = jnp.concatenate(taken, axis=0).astype(jnp.bfloat16)
    down = jnp.concatenate(
        [slot[0:count]] + weights + [jnp.zeros((rows - 2 * count, rows), jnp.float32)], axis=0
    ).T
    fetches[0].wait()
    gate = jnp.dot(taken, gate_ref[...], preferred_element_type=jnp.float32)
    fetches[1].wait()
    up = jnp.dot(taken, up_ref[...], preferred_element_type=jnp.float32)
    hidden = (gate * jax.nn.sigmoid(gate) * up).astype(jnp.bfloat16)
    fetches[2].wait()
    result = jnp.dot(hidden, back_ref[...], preferred_element_type=jnp.float32)
    place = lax.broadcasted_iota(jnp.int32, (rows, region), 1).astype(jnp.float32)
    for i in range(count):
        chosen = (place == down[:, i : i + 1]).astype(jnp.bfloat16)
        spread = jnp.dot(
            chosen,
            result[i * region : (i + 1) * region].astype(jnp.bfloat16),
            preferred_element_type=jnp.float32,
        )
        outs[i][...] = (spread * down[:, count + i : count + i + 1]).astype(jnp.bfloat16)


def run_expert(blocks, own, gate_weight, up_weight, down_weight, capacity):
    rows = blocks[0].shape[0]
    width, hidden = gate_weight.shape
    region = -(-capacity // 8) * 8
    vmem = pl.BlockSpec(memory_space=pltpu.VMEM)
    return pl.pallas_call(
        functools.partial(expert_kernel, region),
        in_specs=[pl.BlockSpec(memory_space=pltpu.SMEM)]
        + [vmem] * len(blocks)
        + [pl.BlockSpec(memory_space=pl.ANY)] * 3,
        out_specs=[vmem] * len(blocks),
        out_shape=[jax.ShapeDtypeStruct((rows, width), jnp.bfloat16)] * len(blocks),
        scratch_shapes=[
            pltpu.VMEM((width, hidden), jnp.bfloat16),
            pltpu.VMEM((width, hidden), jnp.bfloat16),
            pltpu.VMEM((hidden, width), jnp.bfloat16),
            pltpu.SemaphoreType.DMA((3,)),
        ],
        cost_estimate=pl.CostEstimate(
            flops=6 * len(blocks) * region * width * hidden,
            bytes_accessed=6 * width * hidden,
            transcendentals=len(blocks) * region * hidden,
        ),
        name="expert",
    )(own[None], *blocks, gate_weight, up_weight, down_weight)


def added(block, *received):
    if len(received) == 1:
        return block + received[0]
    total = block.astype(jnp.float32)
    for other in received:
        if other is not None:
            total = total + other.astype(jnp.float32)
    return total.astype(jnp.bfloat16)


def stream_kernel(
    residual_ref, own_ref, one_ref, two_ref, three_ref, gain_ref, facts_ref, stream_ref, rows_ref
):
    total = own_ref[...].astype(jnp.float32) + residual_ref[...].astype(jnp.float32)
    for ref in (one_ref, two_ref, three_ref):
        total = total + ref[...].astype(jnp.float32)
    stream = total.astype(jnp.bfloat16)
    stream_ref[...] = stream
    wide = stream.astype(jnp.float32)
    scale = lax.rsqrt(jnp.mean(wide * wide, axis=1, keepdims=True) + EPSILON)
    width = wide.shape[1]
    rows_ref[:, :width] = (wide * scale * gain_ref[...]).astype(jnp.bfloat16)
    rows_ref[:, width:] = facts_ref[...]


def stream_and_rows(residual, parts, gain, token_expert_choice, expert_output_weight):
    rows, width = residual.shape
    high = expert_output_weight.astype(jnp.bfloat16)
    low = (expert_output_weight - high.astype(jnp.float32)).astype(jnp.bfloat16)
    facts = jnp.concatenate([token_expert_choice.astype(jnp.bfloat16), high, low], axis=1)
    facts = jnp.pad(facts, ((0, 0), (0, rows - facts.shape[1])))
    return pl.pallas_call(
        stream_kernel,
        out_shape=[
            jax.ShapeDtypeStruct((rows, width), jnp.bfloat16),
            jax.ShapeDtypeStruct((rows, width + rows), jnp.bfloat16),
        ],
        name="stream",
    )(residual, *parts, gain[None], facts)


SWAPS = [(0, 1), (1, 0), (2, 3), (3, 2)]
MIDDLE = [(1, 2), (2, 1)]
ENDS = [(0, 3), (3, 0)]
OUTWARD = [(1, 0), (2, 3)]
INWARD = [(0, 1), (3, 2)]
MASKS = (0, 1, 3, 2)


def line_sum(parts):
    ends = lax.ppermute(parts[2], "tp", ENDS)
    middle = lax.ppermute(parts[3], "tp", MIDDLE)
    inward = lax.ppermute(parts[3], "tp", INWARD)
    pair = lax.ppermute(added(parts[1], middle), "tp", SWAPS)
    middle_two = lax.ppermute(added(parts[2], inward), "tp", MIDDLE)
    return parts[0], ends, pair, middle_two


def final_kernel(stream_ref, *refs):
    out_ref = refs[-1]
    total = stream_ref[...].astype(jnp.float32)
    for ref in refs[:-1]:
        total = total + ref[...].astype(jnp.float32)
    out_ref[...] = total.astype(jnp.bfloat16)


def near_kernel_sum(keep_ref, back_ref, out_ref):
    total = keep_ref[...].astype(jnp.float32) + back_ref[...].astype(jnp.float32)
    out_ref[...] = total.astype(jnp.bfloat16)


def near_added(keep, back):
    return pl.pallas_call(
        near_kernel_sum,
        out_shape=jax.ShapeDtypeStruct(keep.shape, jnp.bfloat16),
        name="near_sum",
    )(keep, back)


def dense_experts(stream, normed, gate_weight, up_weight, down_weight):
    rows = normed.shape[0]
    capacity = 2 * rows // lax.axis_size("sp") + 1
    place = lax.axis_index("tp")
    mine = lax.axis_index("sp").astype(jnp.int32)
    inner = (place == 1) | (place == 2)

    far = [swapped(normed, 2)]
    from_pair = lax.ppermute(normed, "tp", SWAPS)
    second = lax.ppermute(normed, "tp", MIDDLE + ENDS)
    middle_two = lax.ppermute(from_pair, "tp", MIDDLE)
    outer_two = lax.ppermute(second, "tp", OUTWARD)
    third = jnp.where(inner, middle_two, outer_two)
    blocks = [normed, from_pair, second, third]
    sums = []
    near_other, far_other = [], []
    for turn in range(4):
        if turn:
            far.append(swapped(blocks[turn], 2))
        near_other.append(swapped(blocks[turn], 1))
        far_other.append(swapped(far[turn], 1))
    experts = (mine, gate_weight, up_weight, down_weight, capacity)
    near, crossed = [], []
    for turns in ((0, 1), (2,), (3,)):
        kept = [b for turn in turns for b in (blocks[turn], far[turn])]
        sent = [b for turn in turns for b in (near_other[turn], far_other[turn])]
        results = run_expert(kept + sent, *experts)
        for i, turn in enumerate(turns):
            keep_near, keep_far = results[2 * i : 2 * i + 2]
            send_near, send_far = results[len(kept) + 2 * i : len(kept) + 2 * i + 2]
            back_far = swapped(send_far, 1)
            back_near = swapped(send_near, 1)
            near.append((keep_near, back_near))
            crossed.append(swapped(added(keep_far, back_far), 2))
    near_last = near_added(*near[3])
    parts = [None]
    for turn in (1, 2):
        parts.append(added(*near[turn], crossed[turn]))
    parts[2] = lax.optimization_barrier(parts[2])
    parts.append(lax.optimization_barrier(added(near_last, crossed[3])))
    sums = line_sum(parts)[1:]
    return pl.pallas_call(
        final_kernel,
        out_shape=jax.ShapeDtypeStruct(stream.shape, jnp.bfloat16),
        name="final",
    )(stream, *near[0], crossed[0], *sums)


def local(
    residual,
    grouped_value_heads,
    output_gate_heads,
    projected_key_query,
    raw_step_size,
    step_size_bias,
    head_decay_logarithm,
    position_extra_decay,
    head_skip_weight,
    value_kernel_taps,
    key_query_kernel,
    head_norm_gain,
    output_matrix,
    expert_norm_gain,
    expert_gate_weight,
    expert_up_weight,
    expert_down_weight,
    token_expert_choice,
    expert_output_weight,
):
    lane_width = grouped_value_heads.shape[2]
    dense = lax.axis_size("sp") == 4 and lax.axis_size("tp") == 4
    order = lax.axis_index("tp").astype(jnp.int32) if dense else None
    mixed_heads = mixed_rows(
        grouped_value_heads,
        output_gate_heads,
        projected_key_query,
        raw_step_size,
        step_size_bias,
        head_decay_logarithm,
        position_extra_decay,
        head_skip_weight,
        value_kernel_taps,
        key_query_kernel,
        head_norm_gain,
        output_matrix,
        order,
    )
    weights = (expert_gate_weight[0], expert_up_weight[0], expert_down_weight[0])
    if dense:
        stream, normed = stream_and_rows(
            residual,
            line_sum(mixed_heads),
            expert_norm_gain,
            token_expert_choice,
            expert_output_weight,
        )
        return dense_experts(stream, normed, *weights)
    model_width = output_matrix.shape[2]
    mix_out = lax.psum_scatter(
        jnp.dot(
            mixed_heads,
            output_matrix.reshape(2 * lane_width, model_width),
            preferred_element_type=jnp.float32,
        ).astype(jnp.bfloat16),
        "tp",
        scatter_dimension=0,
        tiled=True,
    ).astype(jnp.float32)
    stream = (residual.astype(jnp.float32) + mix_out).astype(jnp.bfloat16)
    wide_stream = stream.astype(jnp.float32)
    normed = (
        wide_stream
        * lax.rsqrt(jnp.mean(wide_stream * wide_stream, axis=1, keepdims=True) + EPSILON)
        * expert_norm_gain[None]
    ).astype(jnp.bfloat16)
    return routed_experts(wide_stream, normed, *weights, token_expert_choice, expert_output_weight)


def solution(mesh):
    placed = (
        P(("grp", "sp", "tp"), None),
        P(("grp", "sp"), None, "tp"),
        P(("grp", "sp"), None, "tp"),
        P(("grp", "sp"), None),
        P(("grp", "sp"), None, "tp"),
        P(None, "tp"),
        P(None, "tp"),
        P(("grp", "sp")),
        P(None, "tp"),
        P(None, None, "tp"),
        P(),
        P(None, "tp"),
        P(None, "tp", None),
        P(),
        P("sp", None, "tp"),
        P("sp", None, "tp"),
        P("sp", "tp", None),
        P(("grp", "sp", "tp"), None),
        P(("grp", "sp", "tp"), None),
    )

    return jax.shard_map(
        local, mesh=mesh, in_specs=placed, out_specs=P(("grp", "sp", "tp"), None), check_vma=False
    )
```

```python
import functools

import jax
import jax.numpy as jnp
from jax import lax
from jax.experimental import pallas as pl
from jax.experimental.pallas import tpu as pltpu
from jax.sharding import PartitionSpec as P


HEAD_DIM = 64
STATE_ONE = 64
STATE_TWO = 128
BLOCK = 128


EPSILON = 1e-06


def passed_along(shard, axis, by):
    length = lax.axis_size(axis)
    pairs = [(i, i + by) for i in range(length) if 0 <= i + by < length]
    return lax.ppermute(shard, axis, pairs)


def high_rows(heads):
    return -(-2 * heads // 8) * 8


def widened(column, heads, width):
    rows = column.shape[0]
    return jnp.concatenate(
        [jnp.broadcast_to(column[:, h : h + 1], (rows, width)) for h in range(heads)], axis=1
    )


def spread_down(tall, first, heads, width):
    return jnp.concatenate(
        [jnp.broadcast_to(tall[first + h : first + h + 1], (1, width)) for h in range(heads)], axis=1
    )


def both_groups(tall, heads, width):
    return jnp.concatenate(
        [spread_down(tall, g * heads, heads, width) for g in range(2)], axis=1
    )


def head_facts(facts_ref, kind, high):
    heads = facts_ref.shape[1]
    both = jnp.concatenate(
        [facts_ref[2 * kind : 2 * kind + 1], facts_ref[2 * kind + 1 : 2 * kind + 2]], axis=1
    )
    if high > 2 * heads:
        both = jnp.concatenate([both, jnp.zeros((1, high - 2 * heads), jnp.float32)], axis=1)
    same = lax.broadcasted_iota(jnp.int32, (high, high), 0) == lax.broadcasted_iota(
        jnp.int32, (high, high), 1
    )
    return jnp.sum(jnp.where(same, jnp.broadcast_to(both, (high, high)), 0.0), axis=1, keepdims=True)


def states_kernel(
    heads,
    sizes,
    values_ref,
    keys_ref,
    rim_ref,
    value_taps_ref,
    key_taps_ref,
    steps_ref,
    facts_ref,
    extra_ref,
    x_ref,
    rows_ref,
    across_ref,
    down_ref,
    enter_one_ref,
    enter_two_ref,
    earlier_ref,
    packed_ref,
    tail_ref,
    one_ref,
    two_ref,
    sum_ref,
):
    step = pl.program_id(0)
    lanes = heads * HEAD_DIM
    taps = value_taps_ref.shape[0]

    @pl.when(step == 0)
    def _():
        tail_ref[...] = rim_ref[...].astype(jnp.float32)
        one_ref[...] = jnp.zeros_like(one_ref)
        two_ref[...] = jnp.zeros_like(two_ref)
        sum_ref[...] = jnp.zeros_like(sum_ref)

    here = jnp.concatenate(
        [values_ref[:, g].astype(jnp.float32) for g in range(2)]
        + [keys_ref[...].astype(jnp.float32)],
        axis=1,
    )
    extended = jnp.concatenate([tail_ref[...], here], axis=0)
    tail_ref[...] = here[BLOCK - 8 :]
    weights = jnp.concatenate(
        [value_taps_ref[:, g].astype(jnp.float32) for g in range(2)]
        + [key_taps_ref[...].astype(jnp.float32)],
        axis=1,
    )
    summed = jnp.zeros_like(here)
    for j in range(taps):
        first = 8 - (taps - 1) + j
        summed = summed + extended[first : first + BLOCK] * weights[j : j + 1]
    active = (summed * jax.nn.sigmoid(summed)).astype(jnp.bfloat16)
    x = active[:, : 2 * lanes]
    rows = active[:, 2 * lanes :]
    x_ref[...] = x
    rows_ref[...] = rows

    high = high_rows(heads)
    raw = [steps_ref[g].astype(jnp.float32) for g in range(2)]
    if high > 2 * heads:
        raw.append(jnp.zeros((high - 2 * heads, BLOCK), jnp.float32))
    raw = jnp.concatenate(raw, axis=0) + head_facts(facts_ref, 0, high)
    stride = jnp.maximum(raw, 0.0) + jnp.log1p(jnp.exp(-jnp.abs(raw)))
    log_decay = extra_ref[...] - jnp.exp(head_facts(facts_ref, 1, high)) * stride
    upto = (
        lax.broadcasted_iota(jnp.int32, (BLOCK, BLOCK), 0)
        <= lax.broadcasted_iota(jnp.int32, (BLOCK, BLOCK), 1)
    ).astype(jnp.float32)
    running = jnp.dot(
        log_decay, upto, preferred_element_type=jnp.float32, precision=lax.Precision.HIGHEST
    )
    end = running[:, BLOCK - 1 :]
    fading = jnp.exp(end - running) * stride
    stacked = jnp.concatenate(
        [running, fading, jnp.exp(running)]
        + [jnp.zeros((BLOCK - 3 * high, BLOCK), jnp.float32)],
        axis=0,
    )
    down = stacked.T
    across_ref[...] = jnp.concatenate([running, stride], axis=0)
    down_ref[...] = down
    earlier_ref[...] = jnp.broadcast_to(
        jnp.exp(both_groups(sum_ref[...], heads, HEAD_DIM)), earlier_ref.shape
    )
    faded_end = jnp.exp(both_groups(end, heads, HEAD_DIM))
    bound = 0
    for g, (enter_ref, state_ref) in enumerate(((enter_one_ref, one_ref), (enter_two_ref, two_ref))):
        keys = rows[:, bound : bound + sizes[g]]
        bound += 2 * sizes[g]
        fade = widened(down[:, high + g * heads : high + (g + 1) * heads], heads, HEAD_DIM)
        scaled = (x[:, g * lanes : (g + 1) * lanes].astype(jnp.float32) * fade).astype(jnp.bfloat16)
        own = lax.dot_general(
            keys, scaled, (((0,), (0,)), ((), ())), preferred_element_type=jnp.float32
        )
        state = state_ref[...]
        enter_ref[0] = state
        state_ref[...] = state * faded_end[:, g * lanes : (g + 1) * lanes] + own
    total = sum_ref[...] + end
    sum_ref[...] = total

    @pl.when(step == pl.num_programs(0) - 1)
    def _():
        whole = both_groups(total, heads, HEAD_DIM)
        high_part = whole.astype(jnp.bfloat16)
        low_part = (whole - high_part.astype(jnp.float32)).astype(jnp.bfloat16)
        packed_ref[0 : sizes[0]] = one_ref[...].astype(jnp.bfloat16)
        packed_ref[sizes[0] : sizes[0] + sizes[1]] = two_ref[...].astype(jnp.bfloat16)
        packed_ref[sizes[0] + sizes[1] :] = jnp.concatenate(
            [
                jnp.broadcast_to(part[:, g * lanes : (g + 1) * lanes].astype(jnp.float32), (4, lanes))
                for g in range(2)
                for part in (high_part, low_part)
            ],
            axis=0,
        ).astype(jnp.bfloat16)


def near_kernel(heads, sizes, x_ref, rows_ref, across_ref, down_ref, facts_ref, near_ref):
    high = across_ref.shape[0] // 2
    later = lax.broadcasted_iota(jnp.int32, (BLOCK, BLOCK), 0) >= lax.broadcasted_iota(
        jnp.int32, (BLOCK, BLOCK), 1
    )
    skip = both_groups(head_facts(facts_ref, 2, high), heads, HEAD_DIM)
    bound = 0
    out = []
    for g in range(2):
        keys = rows_ref[:, bound : bound + sizes[g]]
        queries = rows_ref[:, bound + sizes[g] : bound + 2 * sizes[g]]
        bound += 2 * sizes[g]
        scores = lax.dot_general(
            queries, keys, (((1,), (1,)), ((), ())), preferred_element_type=jnp.float32
        )
        for h in range(heads):
            i = g * heads + h
            spread = jnp.where(later, down_ref[:, i : i + 1] - across_ref[i : i + 1], -1e30)
            weights = scores * jnp.exp(spread) * across_ref[high + i : high + i + 1]
            x = x_ref[:, i * HEAD_DIM : (i + 1) * HEAD_DIM]
            out.append(
                jnp.dot(weights.astype(jnp.bfloat16), x, preferred_element_type=jnp.float32)
            )
    near_ref[...] = jnp.concatenate(out, axis=1) + skip * x_ref[...].astype(jnp.float32)


def mixed_values(heads, sizes, prior_count, refs):
    priors = refs[:prior_count]
    (
        near_ref,
        rows_ref,
        down_ref,
        enter_one_ref,
        enter_two_ref,
        earlier_ref,
        gate_ref,
        gain_ref,
        one_ref,
        two_ref,
    ) = refs[prior_count:]
    lanes = heads * HEAD_DIM
    high = high_rows(heads)

    @pl.when(pl.program_id(0) == 0)
    def _():
        base = sizes[0] + sizes[1]
        for g, state_ref in enumerate((one_ref, two_ref)):
            state = jnp.zeros_like(state_ref)
            first = g * sizes[0]
            for prior in reversed(priors):
                facts = prior[base:].astype(jnp.float32)
                decay = facts[8 * g : 8 * g + 1] + facts[8 * g + 4 : 8 * g + 5]
                own = prior[first : first + sizes[g]].astype(jnp.float32)
                state = state * jnp.exp(decay) + own
            state_ref[...] = state

    bound = 0
    out = []
    for g, (enter_ref, state_ref) in enumerate(((enter_one_ref, one_ref), (enter_two_ref, two_ref))):
        queries = rows_ref[:, bound + sizes[g] : bound + 2 * sizes[g]]
        bound += 2 * sizes[g]
        here = slice(g * lanes, (g + 1) * lanes)
        entering = enter_ref[0] + state_ref[...] * earlier_ref[0:1, here]
        far = jnp.dot(
            queries, entering.astype(jnp.bfloat16), preferred_element_type=jnp.float32
        )
        reach = down_ref[:, 2 * high + g * heads : 2 * high + (g + 1) * heads]
        gate = gate_ref[:, g].astype(jnp.float32)
        total = near_ref[:, here] + far * widened(reach, heads, HEAD_DIM)
        gated = total * (gate * jax.nn.sigmoid(gate))
        squares = gated * gated
        means = jnp.concatenate(
            [
                jnp.sum(squares[:, h * HEAD_DIM : (h + 1) * HEAD_DIM], axis=1, keepdims=True)
                for h in range(heads)
            ],
            axis=1,
        ) * (1.0 / HEAD_DIM)
        scale = widened(lax.rsqrt(means + EPSILON), heads, HEAD_DIM)
        out.append((gated * scale * gain_ref[g : g + 1]).astype(jnp.bfloat16))
    return jnp.concatenate(out, axis=1)


def mixed_kernel(heads, sizes, prior_count, *refs):
    inputs = prior_count + 8
    refs[inputs][...] = mixed_values(heads, sizes, prior_count, refs[:inputs] + refs[inputs + 1 :])


def projected_kernel(heads, sizes, prior_count, turns, order_ref, *refs):
    inputs = prior_count + 8
    matrix_ref, outs = refs[inputs], refs[inputs + 1 : inputs + 1 + turns]
    mixed = mixed_values(heads, sizes, prior_count, refs[:inputs] + refs[inputs + 1 + turns :])
    product = jnp.dot(mixed, matrix_ref[...], preferred_element_type=jnp.float32)
    for turn, out_ref in enumerate(outs):

        @pl.when(pl.program_id(0) == turn)
        def _(out_ref=out_ref):
            out_ref[...] = product.astype(jnp.bfloat16)


def mixed_rows(
    grouped_value_heads,
    output_gate_heads,
    projected_key_query,
    raw_step_size,
    step_size_bias,
    head_decay_logarithm,
    position_extra_decay,
    head_skip_weight,
    value_kernel_taps,
    key_query_kernel,
    head_norm_gain,
    output_matrix,
    order,
):
    positions, _, lanes = grouped_value_heads.shape
    heads = lanes // HEAD_DIM
    high = high_rows(heads)
    sizes = (STATE_ONE, STATE_TWO)
    width = key_query_kernel.shape[1]
    blocks = positions // BLOCK
    last = grouped_value_heads[positions - 8 :].reshape(8, 2 * lanes)
    rim = passed_along(
        jnp.concatenate([last, projected_key_query[positions - 8 :]], axis=1), "sp", 1
    )
    facts = jnp.concatenate([step_size_bias, head_decay_logarithm, head_skip_weight], axis=0)
    steps = raw_step_size.transpose(1, 2, 0)

    def by_block(rows, columns):
        return pl.BlockSpec((rows, columns), lambda k: (k, 0))

    def along(rows):
        return pl.BlockSpec((rows, BLOCK), lambda k: (0, k))

    def fixed(*shape):
        return pl.BlockSpec(shape, lambda k: (0,) * len(shape))

    def per_block(*shape):
        return pl.BlockSpec((1, *shape), lambda k: (k,) + (0,) * len(shape))

    f32, bf16 = jnp.float32, jnp.bfloat16
    packed_rows = sizes[0] + sizes[1] + 16
    x, rows, across, down, enter_one, enter_two, earlier, packed = pl.pallas_call(
        functools.partial(states_kernel, heads, sizes),
        grid=(blocks,),
        in_specs=[
            pl.BlockSpec((BLOCK, 2, lanes), lambda k: (k, 0, 0)),
            by_block(BLOCK, width),
            fixed(8, 2 * lanes + width),
            fixed(*value_kernel_taps.shape),
            fixed(*key_query_kernel.shape),
            pl.BlockSpec((2, heads, BLOCK), lambda k: (0, 0, k)),
            fixed(6, heads),
            along(1),
        ],
        out_specs=[
            by_block(BLOCK, 2 * lanes),
            by_block(BLOCK, width),
            along(2 * high),
            by_block(BLOCK, BLOCK),
            per_block(sizes[0], lanes),
            per_block(sizes[1], lanes),
            by_block(8, 2 * lanes),
            fixed(packed_rows, lanes),
        ],
        out_shape=[
            jax.ShapeDtypeStruct((positions, 2 * lanes), bf16),
            jax.ShapeDtypeStruct((positions, width), bf16),
            jax.ShapeDtypeStruct((2 * high, positions), f32),
            jax.ShapeDtypeStruct((positions, BLOCK), f32),
            jax.ShapeDtypeStruct((blocks, sizes[0], lanes), f32),
            jax.ShapeDtypeStruct((blocks, sizes[1], lanes), f32),
            jax.ShapeDtypeStruct((8 * blocks, 2 * lanes), f32),
            jax.ShapeDtypeStruct((packed_rows, lanes), bf16),
        ],
        scratch_shapes=[
            pltpu.VMEM((8, 2 * lanes + width), f32),
            pltpu.VMEM((sizes[0], lanes), f32),
            pltpu.VMEM((sizes[1], lanes), f32),
            pltpu.VMEM((high, 1), f32),
        ],
        name="states",
    )(
        grouped_value_heads,
        projected_key_query,
        rim,
        value_kernel_taps,
        key_query_kernel,
        steps,
        facts,
        position_extra_decay[None],
    )
    priors = [passed_along(packed, "sp", by) for by in range(1, lax.axis_size("sp"))]
    near_sizes = functools.partial(near_kernel, heads, sizes)
    near_operands = (x, rows, across, down, facts)
    operands = (
        rows,
        down,
        enter_one,
        enter_two,
        earlier,
        output_gate_heads,
        head_norm_gain,
    )
    scratch_shapes = [pltpu.VMEM((sizes[0], lanes), f32), pltpu.VMEM((sizes[1], lanes), f32)]
    if order is None:
        near = pl.pallas_call(
            near_sizes,
            grid=(blocks,),
            in_specs=[
                by_block(BLOCK, 2 * lanes),
                by_block(BLOCK, width),
                along(2 * high),
                by_block(BLOCK, BLOCK),
                fixed(6, heads),
            ],
            out_specs=by_block(BLOCK, 2 * lanes),
            out_shape=jax.ShapeDtypeStruct((positions, 2 * lanes), f32),
            name="near",
        )(*near_operands)
        return pl.pallas_call(
            functools.partial(mixed_kernel, heads, sizes, len(priors)),
            grid=(blocks,),
            in_specs=[fixed(packed_rows, lanes) for _ in priors]
            + [
                by_block(BLOCK, 2 * lanes),
                by_block(BLOCK, width),
                by_block(BLOCK, BLOCK),
                per_block(sizes[0], lanes),
                per_block(sizes[1], lanes),
                by_block(8, 2 * lanes),
                pl.BlockSpec((BLOCK, 2, lanes), lambda k: (k, 0, 0)),
                fixed(2, lanes),
            ],
            out_specs=by_block(BLOCK, 2 * lanes),
            out_shape=jax.ShapeDtypeStruct((positions, 2 * lanes), bf16),
            scratch_shapes=scratch_shapes,
            name="mixed",
        )(*priors, near, *operands)

    def whole(*shape):
        return pl.BlockSpec(shape, lambda k, order: (0,) * len(shape))

    model_width = output_matrix.shape[2]
    outs = {}
    for turns in ((3, 2), (1, 0)):
        count = len(turns)

        def target(k, order, turns=turns):
            return order[0] ^ jnp.where(k == 0, MASKS[turns[0]], MASKS[turns[1]])

        def chosen(rows, columns, target=target):
            return pl.BlockSpec((rows, columns), lambda k, order: (target(k, order), 0))

        def chosen_state(*shape, target=target):
            rest = (0,) * len(shape)
            return pl.BlockSpec((1, *shape), lambda k, order: (target(k, order), *rest))

        near = pl.pallas_call(
            lambda order_ref, *refs: near_sizes(*refs),
            grid_spec=pltpu.PrefetchScalarGridSpec(
                num_scalar_prefetch=1,
                grid=(count,),
                in_specs=[
                    chosen(BLOCK, 2 * lanes),
                    chosen(BLOCK, width),
                    pl.BlockSpec((2 * high, BLOCK), lambda k, order, t=target: (0, t(k, order))),
                    chosen(BLOCK, BLOCK),
                    whole(6, heads),
                ],
                out_specs=pl.BlockSpec((BLOCK, 2 * lanes), lambda k, order: (k, 0)),
            ),
            out_shape=jax.ShapeDtypeStruct((count * BLOCK, 2 * lanes), f32),
            name="near",
        )(order[None], *near_operands)
        results = pl.pallas_call(
            functools.partial(projected_kernel, heads, sizes, len(priors), count),
            grid_spec=pltpu.PrefetchScalarGridSpec(
                num_scalar_prefetch=1,
                grid=(count,),
                in_specs=[whole(packed_rows, lanes) for _ in priors]
                + [
                    pl.BlockSpec((BLOCK, 2 * lanes), lambda k, order: (k, 0)),
                    chosen(BLOCK, width),
                    chosen(BLOCK, BLOCK),
                    chosen_state(sizes[0], lanes),
                    chosen_state(sizes[1], lanes),
                    chosen(8, 2 * lanes),
                    pl.BlockSpec((BLOCK, 2, lanes), lambda k, order, t=target: (t(k, order), 0, 0)),
                    whole(2, lanes),
                    whole(2 * lanes, model_width),
                ],
                out_specs=[whole(BLOCK, model_width)] * count,
                scratch_shapes=scratch_shapes,
            ),
            out_shape=[jax.ShapeDtypeStruct((BLOCK, model_width), bf16)] * count,
            name="projected",
        )(order[None], *priors, near, *operands, output_matrix.reshape(2 * lanes, model_width))
        outs.update(zip(turns, results))
    return [outs[turn] for turn in range(blocks)]


def routed_experts(
    wide_stream, normed, gate_weight, up_weight, down_weight, token_expert_choice, expert_output_weight
):
    rows_here, model_width = normed.shape
    expert_total = lax.axis_size("sp")
    capacity = 2 * rows_here // expert_total + 1
    flat_ids = token_expert_choice.reshape(-1)
    matches = (flat_ids[:, None] == jnp.arange(expert_total, dtype=jnp.int32)[None, :]).astype(
        jnp.int32
    )
    slot_rank = jnp.sum((jnp.cumsum(matches, axis=0) - matches) * matches, axis=1)
    target = flat_ids * capacity + slot_rank
    outbound = (
        jnp.zeros((expert_total * capacity, model_width), jnp.bfloat16)
        .at[target]
        .set(jnp.repeat(normed, 2, axis=0))
    )
    outbound = outbound.reshape(expert_total, capacity, model_width)
    widened = lax.all_gather(
        lax.all_to_all(outbound, "sp", split_axis=0, concat_axis=0, tiled=True),
        "tp",
        axis=0,
        tiled=True,
    )
    flat_rows = widened.reshape(-1, widened.shape[-1])
    gate_out = jnp.dot(flat_rows, gate_weight, preferred_element_type=jnp.float32)
    up_out = jnp.dot(flat_rows, up_weight, preferred_element_type=jnp.float32)
    hidden = (jax.nn.silu(gate_out) * up_out).astype(jnp.bfloat16)
    partial_value = jnp.dot(
        hidden, down_weight, preferred_element_type=jnp.float32
    ).astype(jnp.bfloat16)
    partial_value = lax.optimization_barrier(
        partial_value.reshape(widened.shape[0], widened.shape[1], partial_value.shape[-1])
    ).astype(jnp.float32)
    summed = lax.psum_scatter(
        partial_value.astype(jnp.bfloat16), "tp", scatter_dimension=0, tiled=True
    )
    returned = lax.all_to_all(summed, "sp", split_axis=0, concat_axis=0, tiled=True)
    picked = jnp.take(returned.reshape(expert_total * capacity, model_width), target, axis=0)
    picked = picked.reshape(rows_here, 2, model_width).astype(jnp.float32)
    weighted = (
        expert_output_weight[:, 0:1] * picked[:, 0] + expert_output_weight[:, 1:2] * picked[:, 1]
    )
    return (wide_stream + weighted).astype(jnp.bfloat16)


def swapped(array, bit):
    return lax.ppermute(array, "sp", [(i, i ^ bit) for i in range(lax.axis_size("sp"))])


def expert_kernel(region, own_ref, *refs):
    count = (len(refs) - 7) // 2
    blocks = refs[:count]
    outs = refs[count + 3 : 2 * count + 3]
    gate_ref, up_ref, back_ref, arrived = refs[2 * count + 3 :]
    fetches = [
        pltpu.make_async_copy(source, target, arrived.at[i])
        for i, (source, target) in enumerate(zip(refs[count : count + 3], (gate_ref, up_ref, back_ref)))
    ]
    fetches[0].start()
    fetches[1].start()
    width = gate_ref.shape[0]
    rows = blocks[0].shape[0]
    own = own_ref[0].astype(jnp.float32)
    place = lax.broadcasted_iota(jnp.int32, (region, rows), 0).astype(jnp.float32)
    before = (
        lax.broadcasted_iota(jnp.int32, (rows, rows), 0)
        < lax.broadcasted_iota(jnp.int32, (rows, rows), 1)
    ).astype(jnp.float32)
    named, weights = [], []
    for block in blocks:
        facts = block[:, width:].astype(jnp.float32).T
        hits = (facts[0:2] == own).astype(jnp.float32)
        named.append(hits[0:1] + hits[1:2])
        weights.append(
            hits[0:1] * (facts[2:3] + facts[4:5]) + hits[1:2] * (facts[3:4] + facts[5:6])
        )
    named = jnp.concatenate(named + named[: max(8 - count, 0)], axis=0)
    inner = jnp.dot(named, before, preferred_element_type=jnp.float32)
    slot = jnp.where(named > 0, inner, -1.0)
    taken = []
    for i, block in enumerate(blocks):
        chosen = (place == slot[i : i + 1]).astype(jnp.bfloat16)
        taken.append(jnp.dot(chosen, block[:, :width], preferred_element_type=jnp.float32))
    taken = jnp.concatenate(taken, axis=0).astype(jnp.bfloat16)
    down = jnp.concatenate(
        [slot[0:count]] + weights + [jnp.zeros((rows - 2 * count, rows), jnp.float32)], axis=0
    ).T
    fetches[0].wait()
    fetches[2].start()
    gate = jnp.dot(taken, gate_ref[...], preferred_element_type=jnp.float32)
    fetches[1].wait()
    up = jnp.dot(taken, up_ref[...], preferred_element_type=jnp.float32)
    hidden = (gate * jax.nn.sigmoid(gate) * up).astype(jnp.bfloat16)
    fetches[2].wait()
    result = jnp.dot(hidden, back_ref[...], preferred_element_type=jnp.float32)
    place = lax.broadcasted_iota(jnp.int32, (rows, region), 1).astype(jnp.float32)
    for i in range(count):
        chosen = (place == down[:, i : i + 1]).astype(jnp.bfloat16)
        spread = jnp.dot(
            chosen,
            result[i * region : (i + 1) * region].astype(jnp.bfloat16),
            preferred_element_type=jnp.float32,
        )
        outs[i][...] = (spread * down[:, count + i : count + i + 1]).astype(jnp.bfloat16)


def run_expert(blocks, own, gate_weight, up_weight, down_weight, capacity):
    rows = blocks[0].shape[0]
    width, hidden = gate_weight.shape
    region = -(-capacity // 8) * 8
    vmem = pl.BlockSpec(memory_space=pltpu.VMEM)
    return pl.pallas_call(
        functools.partial(expert_kernel, region),
        in_specs=[pl.BlockSpec(memory_space=pltpu.SMEM)]
        + [vmem] * len(blocks)
        + [pl.BlockSpec(memory_space=pl.ANY)] * 3,
        out_specs=[vmem] * len(blocks),
        out_shape=[jax.ShapeDtypeStruct((rows, width), jnp.bfloat16)] * len(blocks),
        scratch_shapes=[
            pltpu.VMEM((width, hidden), jnp.bfloat16),
            pltpu.VMEM((width, hidden), jnp.bfloat16),
            pltpu.VMEM((hidden, width), jnp.bfloat16),
            pltpu.SemaphoreType.DMA((3,)),
        ],
        cost_estimate=pl.CostEstimate(
            flops=6 * len(blocks) * region * width * hidden,
            bytes_accessed=6 * width * hidden,
            transcendentals=len(blocks) * region * hidden,
        ),
        name="expert",
    )(own[None], *blocks, gate_weight, up_weight, down_weight)


def added(block, *received):
    if len(received) == 1:
        return block + received[0]
    total = block.astype(jnp.float32)
    for other in received:
        if other is not None:
            total = total + other.astype(jnp.float32)
    return total.astype(jnp.bfloat16)


def stream_kernel(
    residual_ref, own_ref, one_ref, two_ref, three_ref, gain_ref, facts_ref, stream_ref, rows_ref
):
    total = own_ref[...].astype(jnp.float32) + residual_ref[...].astype(jnp.float32)
    for ref in (one_ref, two_ref, three_ref):
        total = total + ref[...].astype(jnp.float32)
    stream = total.astype(jnp.bfloat16)
    stream_ref[...] = stream
    wide = stream.astype(jnp.float32)
    scale = lax.rsqrt(jnp.mean(wide * wide, axis=1, keepdims=True) + EPSILON)
    width = wide.shape[1]
    rows_ref[:, :width] = (wide * scale * gain_ref[...]).astype(jnp.bfloat16)
    rows_ref[:, width:] = facts_ref[...]


def stream_and_rows(residual, parts, gain, token_expert_choice, expert_output_weight):
    rows, width = residual.shape
    high = expert_output_weight.astype(jnp.bfloat16)
    low = (expert_output_weight - high.astype(jnp.float32)).astype(jnp.bfloat16)
    facts = jnp.concatenate([token_expert_choice.astype(jnp.bfloat16), high, low], axis=1)
    facts = jnp.pad(facts, ((0, 0), (0, rows - facts.shape[1])))
    return pl.pallas_call(
        stream_kernel,
        out_shape=[
            jax.ShapeDtypeStruct((rows, width), jnp.bfloat16),
            jax.ShapeDtypeStruct((rows, width + rows), jnp.bfloat16),
        ],
        name="stream",
    )(residual, *parts, gain[None], facts)


SWAPS = [(0, 1), (1, 0), (2, 3), (3, 2)]
MIDDLE = [(1, 2), (2, 1)]
ENDS = [(0, 3), (3, 0)]
OUTWARD = [(1, 0), (2, 3)]
INWARD = [(0, 1), (3, 2)]
MASKS = (0, 1, 3, 2)


def line_sum(parts):
    ends = lax.ppermute(parts[2], "tp", ENDS)
    middle = lax.ppermute(parts[3], "tp", MIDDLE)
    inward = lax.ppermute(parts[3], "tp", INWARD)
    pair = lax.ppermute(added(parts[1], middle), "tp", SWAPS)
    middle_two = lax.ppermute(added(parts[2], inward), "tp", MIDDLE)
    return parts[0], ends, pair, middle_two


def final_kernel(stream_ref, *refs):
    out_ref = refs[-1]
    total = stream_ref[...].astype(jnp.float32)
    for ref in refs[:-1]:
        total = total + ref[...].astype(jnp.float32)
    out_ref[...] = total.astype(jnp.bfloat16)


def near_kernel_sum(keep_ref, back_ref, out_ref):
    total = keep_ref[...].astype(jnp.float32) + back_ref[...].astype(jnp.float32)
    out_ref[...] = total.astype(jnp.bfloat16)


def near_added(keep, back):
    return pl.pallas_call(
        near_kernel_sum,
        out_shape=jax.ShapeDtypeStruct(keep.shape, jnp.bfloat16),
        name="near_sum",
    )(keep, back)


def dense_experts(stream, normed, gate_weight, up_weight, down_weight):
    rows = normed.shape[0]
    capacity = 2 * rows // lax.axis_size("sp") + 1
    place = lax.axis_index("tp")
    mine = lax.axis_index("sp").astype(jnp.int32)
    inner = (place == 1) | (place == 2)

    far = [swapped(normed, 2)]
    from_pair = lax.ppermute(normed, "tp", SWAPS)
    second = lax.ppermute(normed, "tp", MIDDLE + ENDS)
    middle_two = lax.ppermute(from_pair, "tp", MIDDLE)
    outer_two = lax.ppermute(second, "tp", OUTWARD)
    third = jnp.where(inner, middle_two, outer_two)
    blocks = [normed, from_pair, second, third]
    sums = []
    near_other, far_other = [], []
    for turn in range(4):
        if turn:
            far.append(swapped(blocks[turn], 2))
        near_other.append(swapped(blocks[turn], 1))
        far_other.append(swapped(far[turn], 1))
    experts = (mine, gate_weight, up_weight, down_weight, capacity)
    near, crossed = [], []
    for turns in ((0, 1), (2,), (3,)):
        kept = [b for turn in turns for b in (blocks[turn], far[turn])]
        sent = [b for turn in turns for b in (near_other[turn], far_other[turn])]
        results = run_expert(kept + sent, *experts)
        for i, turn in enumerate(turns):
            keep_near, keep_far = results[2 * i : 2 * i + 2]
            send_near, send_far = results[len(kept) + 2 * i : len(kept) + 2 * i + 2]
            back_far = swapped(send_far, 1)
            back_near = swapped(send_near, 1)
            near.append((keep_near, back_near))
            crossed.append(swapped(added(keep_far, back_far), 2))
    near_last = near_added(*near[3])
    parts = [None]
    for turn in (1, 2):
        parts.append(added(*near[turn], crossed[turn]))
    parts[2] = lax.optimization_barrier(parts[2])
    parts.append(lax.optimization_barrier(added(near_last, crossed[3])))
    sums = line_sum(parts)[1:]
    return pl.pallas_call(
        final_kernel,
        out_shape=jax.ShapeDtypeStruct(stream.shape, jnp.bfloat16),
        name="final",
    )(stream, *near[0], crossed[0], *sums)


def local(
    residual,
    grouped_value_heads,
    output_gate_heads,
    projected_key_query,
    raw_step_size,
    step_size_bias,
    head_decay_logarithm,
    position_extra_decay,
    head_skip_weight,
    value_kernel_taps,
    key_query_kernel,
    head_norm_gain,
    output_matrix,
    expert_norm_gain,
    expert_gate_weight,
    expert_up_weight,
    expert_down_weight,
    token_expert_choice,
    expert_output_weight,
):
    lane_width = grouped_value_heads.shape[2]
    dense = lax.axis_size("sp") == 4 and lax.axis_size("tp") == 4
    order = lax.axis_index("tp").astype(jnp.int32) if dense else None
    mixed_heads = mixed_rows(
        grouped_value_heads,
        output_gate_heads,
        projected_key_query,
        raw_step_size,
        step_size_bias,
        head_decay_logarithm,
        position_extra_decay,
        head_skip_weight,
        value_kernel_taps,
        key_query_kernel,
        head_norm_gain,
        output_matrix,
        order,
    )
    weights = (expert_gate_weight[0], expert_up_weight[0], expert_down_weight[0])
    if dense:
        stream, normed = stream_and_rows(
            residual,
            line_sum(mixed_heads),
            expert_norm_gain,
            token_expert_choice,
            expert_output_weight,
        )
        return dense_experts(stream, normed, *weights)
    model_width = output_matrix.shape[2]
    mix_out = lax.psum_scatter(
        jnp.dot(
            mixed_heads,
            output_matrix.reshape(2 * lane_width, model_width),
            preferred_element_type=jnp.float32,
        ).astype(jnp.bfloat16),
        "tp",
        scatter_dimension=0,
        tiled=True,
    ).astype(jnp.float32)
    stream = (residual.astype(jnp.float32) + mix_out).astype(jnp.bfloat16)
    wide_stream = stream.astype(jnp.float32)
    normed = (
        wide_stream
        * lax.rsqrt(jnp.mean(wide_stream * wide_stream, axis=1, keepdims=True) + EPSILON)
        * expert_norm_gain[None]
    ).astype(jnp.bfloat16)
    return routed_experts(wide_stream, normed, *weights, token_expert_choice, expert_output_weight)


def solution(mesh):
    placed = (
        P(("grp", "sp", "tp"), None),
        P(("grp", "sp"), None, "tp"),
        P(("grp", "sp"), None, "tp"),
        P(("grp", "sp"), None),
        P(("grp", "sp"), None, "tp"),
        P(None, "tp"),
        P(None, "tp"),
        P(("grp", "sp")),
        P(None, "tp"),
        P(None, None, "tp"),
        P(),
        P(None, "tp"),
        P(None, "tp", None),
        P(),
        P("sp", None, "tp"),
        P("sp", None, "tp"),
        P("sp", "tp", None),
        P(("grp", "sp", "tp"), None),
        P(("grp", "sp", "tp"), None),
    )

    return jax.shard_map(
        local, mesh=mesh, in_specs=placed, out_specs=P(("grp", "sp", "tp"), None), check_vma=False
    )
```
